512 devices in a mesh: ep: 32 (over z, core), tp: 16 (over y, x).
Axes of the slice: x: 4, y: 4, z: 16, core: 2. Of those that a mesh axis runs over, the one named last changes fastest.
Arguments:
- queries: bfloat16 [16384, 1024], P('ep', 'tp'), may hold values from -9 to 9
- keys: bfloat16 [16384, 128], P('ep'), may hold values from -6 to 6
- values: bfloat16 [16384, 128], P('ep'), may hold values from -6 to 6
- sink_logits: float32 [16], P('tp'), may hold values from 2 to 7
- out_weight: bfloat16 [1024, 2048], P(None, 'tp'), may hold values from -0.8984375 to 0.8984375
- expert_input: bfloat16 [8192, 2048], P('ep'), may hold values from -6 to 6
- norm_gain: float32 [2048], replicated, may hold values from 0.1 to 1.9
- routes: int32 [8192, 2], P('ep'), may hold values from 0 to 31, all different within a row; in each aligned block of 256 rows (0 to 255, 256 to 511, ...) at most 32 rows name the same one
- route_weights: float32 [8192, 2], P('ep'), may hold values from 0.1 to 1
- gate_weight: bfloat16 [32, 2048, 4096], P('ep', None, 'tp'), may hold values from -0.125 to 0.125
- up_weight: bfloat16 [32, 2048, 4096], P('ep', None, 'tp'), may hold values from -0.125 to 0.125
- down_weight: bfloat16 [32, 4096, 2048], P('ep', 'tp'), may hold values from -0.09375 to 0.09375
Outputs:
- attn_out: bfloat16 [16384, 2048], P('ep', 'tp')
- expert_out: bfloat16 [8192, 2048], P('ep', 'tp')
The draws below stay inside these ranges and needn't reach their ends.
Inputs may be any that keep to these rules, and one draw needn't show every extreme that they name: `routes`: each row names 2 different experts. Within the rows of one index of ep (aligned blocks of 256 rows) no expert is named by more than 32 rows, and in some blocks one expert is named by exactly 32 rows.
All inputs are finite; a program needn't handle non-finite values.
Results may differ from the reference program's by a relative error of at most 0.015.
Values may be sent and summed in bfloat16 or wider, within the bound.
A program may use at most 64 MiB of HBM per device.

```python
import math
import jax
import jax.numpy as jnp
import numpy as np
from jax import lax

D = 2048
HEADS = 16
KV = 2
HD = 64
WINDOW = 128
FF = 4096
TOPK = 2
TOK_E_DEV = 256
TOK_A = 16384
TOK_E = 8192
EXPERTS = 32
CAP = 32
N_EP = 32
N_TP = 16


def draw_queries(key, part):
    sample = jnp.clip(jax.random.normal(key, (TOK_A, HEADS * HD), jnp.float32) * 1.5, -9.0, 9.0)
    return sample.astype(jnp.bfloat16)


def draw_keys(key, part):
    sample = jnp.clip(jax.random.normal(key, (TOK_A, KV * HD), jnp.float32), -6.0, 6.0)
    return sample.astype(jnp.bfloat16)


def block_levels(key, extent, pieces, least, top_value):
    gain, own = 1.0, jax.random.fold_in(key, 6)
    for axis_at, parts in pieces:
        draws = jnp.exp(jax.random.uniform(jax.random.fold_in(own, axis_at), (parts,), jnp.float32, least / len(pieces), top_value / len(pieces)))
        gain = gain * jnp.repeat(draws, extent[axis_at] // parts).reshape([-1 if axis == axis_at else 1 for axis in range(len(extent))])
    return gain


def deal_out(key, own, number, rows, count, top, limit, lean):
    ranking = jax.random.permutation(key, count)
    packed, usual = shares(count, rows * top, limit, lean, True), shares(count, rows * top, limit, lean, False)
    places = jnp.arange(count)

    def named(lengths, turn):
        used = int((lengths > 0).sum())
        fixed = max(1, used // 4)
        moved = fixed + (places - fixed + turn * (used - fixed)) % max(1, count - fixed)
        return jnp.zeros((count,), jnp.int32).at[ranking[jnp.where(places < fixed, places, moved)]].set(jnp.asarray(lengths, jnp.int32))

    lengths = jnp.where(number % 4 == 0, named(packed, number // 4), named(usual, number - number // 4 - 1))
    mixed = jax.random.permutation(jax.random.fold_in(own, 3), count)
    source_of, receiver = mixed[0:count // 2 * 2:2], mixed[1:count // 2 * 2:2]
    margin = jnp.minimum(lengths[source_of] - 1, limit - lengths[receiver]) // 2
    margin = jnp.where((source_of == ranking[0]) | (receiver == ranking[0]) | (lengths[receiver] == 0), 0, jnp.maximum(margin, 0))
    moved = jax.random.randint(jax.random.fold_in(own, 4), (count // 2,), 0, 1 << 20) % (margin + 1)
    lengths = lengths.at[source_of].add(-moved).at[receiver].add(moved)
    members = jnp.searchsorted(jnp.cumsum(lengths), jnp.arange(rows * top), side="right").astype(jnp.int32)
    table = members.reshape(top, rows).T
    table = table[jax.random.permutation(jax.random.fold_in(own, 1), rows)]
    turn = jax.random.randint(jax.random.fold_in(own, 2), (rows, 1), 0, top)
    return jnp.take_along_axis(table, (jnp.arange(top)[None, :] + turn) % top, axis=1)


def shares(count, total, bound, slope, full):
    loads = [(1 << 20) // math.isqrt(grade ** slope) + 1 for grade in range(1, count + 1)]
    largest = bound if full else min(bound, max(-(-total // count), total * loads[0] // sum(loads)))
    least = 1 if total - largest >= count - 1 else 0
    given, rest = [largest] + [least] * (count - 1), total - largest - least * (count - 1)
    while rest > 0:
        free = [i for i in range(1, count) if given[i] < largest] or [i for i in range(1, count) if given[i] < bound]
        whole, remaining = sum([loads[i] for i in free]), rest
        for i in free:
            addition = min(bound - given[i], max(1, remaining * loads[i] // whole), rest)
            given[i] = given[i] + addition
            rest = rest - addition
    return np.array(given)


def noise(key, extent, width, most, split=(), kind=jnp.bfloat16):
    loudness = block_levels(key, extent, split, -0.22, 0.18) if split else 1.0
    values = jax.random.normal(key, extent, jnp.float32) * width * loudness
    return jnp.minimum(jnp.maximum(values, -most), most).astype(kind)


def setup_inputs(seed: int = 0) -> dict:
    streams_of = jax.random.split(jax.random.key(seed), 13)
    queries = draw_queries(jax.random.fold_in(streams_of[12], 71), 0)
    keys = draw_keys(jax.random.fold_in(streams_of[12], 71), 0)
    values = noise(streams_of[2], (TOK_A, KV * HD), 1.0, 6.0, ((0, 32),))
    sink_logits = jnp.clip(2.0 + 5.0 * jax.random.uniform(streams_of[3], (HEADS,), jnp.float32) ** block_levels(streams_of[3], (HEADS,), ((0, 16),), -0.2, 0.2), 2.0, 7.0)
    out_weight = noise(streams_of[4], (HEADS * HD, D), 0.15, 0.8984375, ((1, 16),))
    expert_input = noise(streams_of[5], (TOK_E, D), 1.0, 6.0, ((0, 32),))
    norm_gain = jnp.clip(1.0 + 0.18 * jax.random.normal(streams_of[6], (D,), jnp.float32), 0.1, 1.9)
    routes_keys = jax.random.split(jax.random.fold_in(streams_of[7], 1), TOK_E // TOK_E_DEV)
    routes_turns = jax.random.permutation(jax.random.fold_in(streams_of[7], 3), TOK_E // TOK_E_DEV)
    routes = jax.vmap(lambda own, number: deal_out(jax.random.fold_in(streams_of[7], 2), own, number, TOK_E_DEV, EXPERTS, TOPK, CAP, 1))(routes_keys, routes_turns).reshape((TOK_E, TOPK))
    route_weights = jnp.clip(0.1 + 0.9 * jax.random.uniform(streams_of[8], (TOK_E, TOPK), jnp.float32) ** block_levels(streams_of[8], (TOK_E, TOPK), ((0, 32),), -0.2, 0.2), 0.1, 1.0)
    gate_weight = noise(streams_of[9], (EXPERTS, D, FF), D ** -0.5, 0.125, ((0, 32), (2, 16)))
    up_weight = noise(streams_of[10], (EXPERTS, D, FF), D ** -0.5, 0.125, ((0, 32), (2, 16)))
    down_weight = noise(streams_of[11], (EXPERTS, FF, D), FF ** -0.5, 0.09375, ((0, 32), (1, 16)))
    return {"queries": queries, "keys": keys, "values": values, "sink_logits": sink_logits, "out_weight": out_weight, "expert_input": expert_input, "norm_gain": norm_gain, "routes": routes, "route_weights": route_weights, "gate_weight": gate_weight, "up_weight": up_weight, "down_weight": down_weight}


rms_eps = 1e-06
mask_value = -1e+30

def rotate_heads(values_in, positions):
    half_dim = values_in.shape[-1] // 2
    inv_freq = 10000.0 ** (-jnp.arange(half_dim, dtype=jnp.float32) * (2.0 / values_in.shape[-1]))
    angles = positions[:, None] * inv_freq[None, :]
    cosine_table = jnp.cos(angles)[:, None, :]
    sine_table = jnp.sin(angles)[:, None, :]
    first_half = values_in[..., :half_dim]
    second_half = values_in[..., half_dim:]
    return jnp.concatenate([first_half * cosine_table - second_half * sine_table, second_half * cosine_table + first_half * sine_table], axis=-1)

def one_head(operands):
    head_query, head_key, head_value, head_sink = operands
    tokens_all = head_query.shape[0]
    blocks = tokens_all // WINDOW
    zero_rim = jnp.zeros((WINDOW, HD), head_key.dtype)

    def band_of(source):
        padded = jnp.concatenate([zero_rim, source], axis=0)
        earlier = padded[:tokens_all].reshape(blocks, WINDOW, HD)
        current = padded[WINDOW:].reshape(blocks, WINDOW, HD)
        return jnp.concatenate([earlier, current], axis=1).astype(jnp.float32)
    query_blocks = head_query.reshape(blocks, WINDOW, HD).astype(jnp.float32)
    scores = jnp.einsum('nqd,nkd->nqk', query_blocks, band_of(head_key)) * HD ** (-0.5)
    block_start = jnp.arange(blocks, dtype=jnp.int32)[:, None, None] * WINDOW
    query_pos = block_start + jnp.arange(WINDOW, dtype=jnp.int32)[None, :, None]
    key_pos = block_start - WINDOW + jnp.arange(2 * WINDOW, dtype=jnp.int32)[None, None, :]
    distance = query_pos - key_pos
    allowed = (distance >= 0) & (distance < WINDOW) & (key_pos >= 0)
    scores = jnp.where(allowed, scores, mask_value)
    row_top = jnp.maximum(lax.optimization_barrier(jnp.max(scores, axis=-1)), head_sink)
    exp_scores = jnp.exp(scores - row_top[..., None])
    row_total = lax.optimization_barrier(jnp.sum(exp_scores, axis=-1)) + jnp.exp(head_sink - row_top)
    weights = (exp_scores / row_total[..., None]).astype(jnp.bfloat16)
    head_mix = jnp.einsum('nqk,nkd->nqd', weights.astype(jnp.float32), band_of(head_value))
    return head_mix.astype(jnp.bfloat16).reshape(tokens_all, HD)

def reference(queries, keys, values, sink_logits, out_weight, expert_input, norm_gain, routes, route_weights, gate_weight, up_weight, down_weight):
    tokens_all = queries.shape[0]
    positions = jnp.arange(tokens_all, dtype=jnp.int32).astype(jnp.float32)
    query_rot = rotate_heads(queries.astype(jnp.float32).reshape(tokens_all, HEADS, HD), positions).astype(jnp.bfloat16)
    key_rot = rotate_heads(keys.astype(jnp.float32).reshape(tokens_all, KV, HD), positions).astype(jnp.bfloat16)
    value_heads = values.reshape(tokens_all, KV, HD)
    group_size = HEADS // KV
    query_t = jnp.transpose(query_rot, (1, 0, 2))
    key_t = jnp.repeat(jnp.transpose(key_rot, (1, 0, 2)), group_size, axis=0)
    value_t = jnp.repeat(jnp.transpose(value_heads, (1, 0, 2)), group_size, axis=0)
    head_outputs = lax.map(one_head, (query_t, key_t, value_t, sink_logits.astype(jnp.float32)))
    head_mix = jnp.transpose(head_outputs, (1, 0, 2)).reshape(tokens_all, HEADS * HD)
    attn_out = jnp.dot(head_mix, out_weight, preferred_element_type=jnp.float32).astype(jnp.bfloat16)
    token_rows = expert_input.shape[0]
    input_wide = expert_input.astype(jnp.float32)
    inv_rms = lax.rsqrt(lax.optimization_barrier(jnp.mean(input_wide * input_wide, axis=-1, keepdims=True)) + rms_eps)
    normed = (input_wide * inv_rms * norm_gain.astype(jnp.float32)[None, :]).astype(jnp.bfloat16)
    grouped = routes.reshape(N_EP, TOK_E_DEV * TOPK).astype(jnp.int32)
    one_hot = (grouped[..., None] == jnp.arange(EXPERTS, dtype=jnp.int32)[None, None, :]).astype(jnp.int32)
    route_rank = lax.optimization_barrier(jnp.sum(jnp.cumsum(one_hot, axis=1) * one_hot, axis=-1)) - 1
    source_block = jnp.arange(N_EP, dtype=jnp.int32)[:, None]
    slot_index = (grouped * (N_EP * CAP) + source_block * CAP + route_rank).reshape(-1).astype(jnp.int32)
    route_token = (jnp.arange(token_rows * TOPK, dtype=jnp.int32) // TOPK).astype(jnp.int32)
    slot_table = jnp.full((EXPERTS * N_EP * CAP,), token_rows, jnp.int32).at[slot_index].set(route_token).reshape(EXPERTS, N_EP * CAP)
    padded = jnp.concatenate([normed, jnp.zeros((1, D), normed.dtype)], axis=0)
    width_block = FF // N_TP

    def one_expert(operands):
        table_row, gate_mat, up_mat, down_mat = operands
        rows_in = padded[table_row]
        gate_acc = jnp.dot(rows_in, gate_mat, preferred_element_type=jnp.float32)
        up_acc = jnp.dot(rows_in, up_mat, preferred_element_type=jnp.float32)
        hidden = (jax.nn.silu(gate_acc) * up_acc).astype(jnp.bfloat16)
        block_parts = jnp.einsum('sjf,jfd->jsd', hidden.reshape(-1, N_TP, width_block).astype(jnp.float32), down_mat.reshape(N_TP, width_block, D).astype(jnp.float32)).astype(jnp.bfloat16)
        return lax.optimization_barrier(jnp.sum(block_parts.astype(jnp.float32), axis=0)).astype(jnp.bfloat16)
    outputs = lax.map(one_expert, (slot_table, gate_weight, up_weight, down_weight))
    picked = outputs.reshape(-1, D)[slot_index].astype(jnp.float32)
    expert_out = lax.optimization_barrier(jnp.sum(picked.reshape(token_rows, TOPK, D) * route_weights.astype(jnp.float32)[..., None], axis=1)).astype(jnp.bfloat16)
    return (attn_out, expert_out)
```

```python
import functools

import jax
import jax.numpy as jnp
import numpy as np
from jax import lax
from jax.experimental import pallas as pl
from jax.experimental.pallas import tpu as pltpu
from jax.sharding import Mesh
from jax.sharding import PartitionSpec as P

HEADS = 16
KV = 2
HD = 64
WINDOW = 128
TP = ("tp_0", "tp_1")
NZ = 16
UNITS = 16
ATT_UNITS = 4
ALL_UNITS = UNITS + ATT_UNITS
SLOTS = 32
EXPERTS = 32
ROWS = 64
D = 2048
FF_HERE = 256
TOK_E = 256
TOK_A = 512
MESH = pl.DeviceIdType.MESH

AG3, AG4, MM, RS2, RS3, FIN = 2, 4, 6, 8, 10, 12

rms_eps = 1e-06
mask_value = -1e30

f32 = jnp.float32
bf16 = jnp.bfloat16


def unit_dz(u):
    j = u // 2
    dist = jnp.where(j < 4, 2 * j + 1, 16 - 2 * j)
    sign = 1 - 2 * (u % 2)
    return jnp.where(u == 9, 0, sign * dist)


def rope_tables():
    lane = np.arange(128) % 32
    freq = 10000.0 ** (-lane * (2.0 / HD))
    sign = np.where(np.arange(128) % 64 < 32, -1.0, 1.0)
    near = np.arange(WINDOW)[:, None] * freq[None, :]
    far = (np.arange(128) * WINDOW)[:, None] * freq[None, :]
    tables = np.stack([np.cos(near), np.sin(near) * sign, np.cos(far), np.sin(far) * sign])
    return tables.astype(np.float32)


def dot(a, b):
    return jnp.dot(a, b, preferred_element_type=f32)


def kernel(
    q_in, k_in, v_in, sink_ref, ow_in, x_in, gain_in, routes_in, rw_in, wg_in, wu_in, wd_in, trig_in,
    attn_ref, eout_ref,
    q_v, k_v, v_v, ow_v, x_v, gain_v, routes_v, rw_v, wg_v, wu_v, wd_v, trig_v,
    nrm, disp, w01, qp, kv, xg, yb, ra, rb, rc, tb, qb, rd, fb, home,
    in_sem, zs, zr, hs, hr, a1s, a1r, a3s, a3r, a4s, a4r, b1s, b1r, b2s, b2r, b3s, b3r, ks, kr,
):
    ep = lax.axis_index("ep")
    y = lax.axis_index("tp_0")
    x = lax.axis_index("tp_1")
    z = ep // 2
    core = ep % 2
    tp = y * 4 + x
    sg = 1 - 2 * core

    barrier = pltpu.get_barrier_semaphore()

    def hello(step, carry):
        pl.semaphore_signal(barrier, inc=1, device_id=((ep + step) % 32, y, x), device_id_type=MESH)
        return carry

    lax.fori_loop(1, 32, hello, 0)
    for k in (1, 2, 3):
        pl.semaphore_signal(barrier, inc=1, device_id=(ep, (y + k) % 4, x), device_id_type=MESH)
        pl.semaphore_signal(barrier, inc=1, device_id=(ep, y, (x + k) % 4), device_id_type=MESH)

    pairs = [
        (routes_in, routes_v), (x_in, x_v), (gain_in, gain_v), (rw_in, rw_v), (trig_in, trig_v), (q_in, q_v),
        (k_in, k_v), (v_in, v_v), (wg_in, wg_v), (wu_in, wu_v), (wd_in, wd_v), (ow_in, ow_v),
    ]
    loads = [pltpu.make_async_copy(a, b, in_sem.at[n]) for n, (a, b) in enumerate(pairs)]
    for load in loads:
        load.start()
    (l_routes, l_x, l_gain, l_rw, l_trig, l_q, l_k, l_v, l_wg, l_wu, l_wd, l_ow) = loads

    l_routes.wait()
    routes = routes_v[...]
    e_iota = lax.broadcasted_iota(jnp.int32, (TOK_E, EXPERTS), 1)
    one0 = (routes[:, 0:1] == e_iota).astype(f32)
    one1 = (routes[:, 1:2] == e_iota).astype(f32)
    t_row = lax.broadcasted_iota(jnp.int32, (TOK_E, TOK_E), 0)
    t_col = lax.broadcasted_iota(jnp.int32, (TOK_E, TOK_E), 1)
    lower = (t_col < t_row).astype(f32).astype(bf16)
    rank = dot(lower, (one0 + one1).astype(bf16))
    rank0 = jnp.sum(one0 * rank, axis=1, keepdims=True)
    rank1 = jnp.sum(one1 * rank, axis=1, keepdims=True)
    eye = (t_col == t_row).astype(f32)
    ones = jnp.ones((16, TOK_E), bf16)

    def as_row(column):
        return dot(ones, (eye * column).astype(bf16))[0:1, :]

    slot_row0 = as_row(routes[:, 0:1].astype(f32)) * float(SLOTS) + as_row(rank0)
    slot_row1 = as_row(routes[:, 1:2].astype(f32)) * float(SLOTS) + as_row(rank1)

    l_x.wait()
    l_gain.wait()
    own_cols = pl.ds(pl.multiple_of(tp * 128, 128), 128)
    gain = gain_v[:, own_cols]

    def norm_rows(n, carry):
        rows = pl.ds(pl.multiple_of(n * 32, 32), 32)
        wide = x_v[rows, :].astype(f32)
        inv = lax.rsqrt(jnp.mean(wide * wide, axis=1, keepdims=True) + rms_eps)
        nrm[rows, :] = (x_v[rows, own_cols].astype(f32) * inv * gain).astype(bf16)
        return carry

    lax.fori_loop(0, 8, norm_rows, 0)
    normed = nrm[...]

    def fill_slots(n, carry):
        slot = (lax.broadcasted_iota(jnp.int32, (256, TOK_E), 0) + n * 256).astype(f32)
        pick = ((slot == slot_row0) | (slot == slot_row1)).astype(f32).astype(bf16)
        disp[pl.ds(n * 8, 8)] = dot(pick, normed).astype(bf16).reshape(8, SLOTS, 128)
        return carry

    lax.fori_loop(0, 4, fill_slots, 0)
    pl.semaphore_wait(barrier, 37)

    def place(u):
        odd = u % 2
        return jnp.where(odd == 1, x, y), jnp.where(odd == 1, y, x)

    def along_j(u, k):
        odd = u % 2
        return (ep, jnp.where(odd == 1, (y + k) % 4, y), jnp.where(odd == 1, x, (x + k) % 4))

    def along_i(u, k):
        odd = u % 2
        return (ep, jnp.where(odd == 1, y, (y + k) % 4), jnp.where(odd == 1, (x + k) % 4, x))

    fw = sg + 4
    bw = 4 - sg

    def z_copy(u, cc):
        dest = ((z - unit_dz(u) + NZ) % NZ) * 2 + cc
        i, j = place(u)
        return pltpu.make_async_remote_copy(
            src_ref=disp.at[dest], dst_ref=xg.at[u, i, j, core],
            send_sem=zs.at[u, cc], recv_sem=zr.at[u, core],
            device_id=(dest, y, x), device_id_type=MESH,
        )

    def z_wait(u, c):
        i, j = place(u)
        pltpu.make_async_remote_copy(
            src_ref=disp.at[0], dst_ref=xg.at[u, i, j, c],
            send_sem=zs.at[u, c], recv_sem=zr.at[u, c],
            device_id=(ep ^ 1, y, x), device_id_type=MESH,
        ).wait_recv()

    def z_send(u, carry):
        for cc in (0, 1):
            @pl.when(jnp.logical_not((u == 9) & (core == cc)))
            def _():
                z_copy(u, cc).start()
        return carry

    lax.fori_loop(0, UNITS, z_send, 0)
    xg[9, x, y, core] = disp[ep]

    l_trig.wait()
    l_q.wait()
    l_k.wait()
    l_v.wait()
    group = y // 2
    lane = lax.broadcasted_iota(jnp.int32, (WINDOW, 128), 1)
    first = lane < HD

    def rotate_block(n, carry):
        rows = pl.ds(pl.multiple_of(n * WINDOW, WINDOW), WINDOW)
        q = q_v[rows, :].astype(f32)
        k = k_v[rows, :].astype(f32)
        v = v_v[rows, :].astype(f32)
        k = jnp.where(group == 0, pltpu.roll(k, HD, 1), k)
        v = jnp.where(group == 0, pltpu.roll(v, HD, 1), v)
        both = jnp.where(first, jnp.concatenate([q, q], axis=1), k)
        block = ep * 4 + n
        cb = trig_v[2, pl.ds(block, 1), :]
        sb = trig_v[3, pl.ds(block, 1), :]
        cr = trig_v[0]
        sr = trig_v[1]
        cos = cb * cr - sb * sr
        sin = sb * cr + cb * sr
        swapped = jnp.where(lane % HD < HD // 2, pltpu.roll(both, 128 - HD // 2, 1), pltpu.roll(both, HD // 2, 1))
        turned = both * cos + swapped * sin
        qp[n] = jnp.where(first, turned, 0.0).astype(bf16)
        kv[n + 1] = jnp.where(first, pltpu.roll(turned, HD, 1), v).astype(bf16)
        return carry

    lax.fori_loop(0, 4, rotate_block, 0)
    rim = pltpu.make_async_remote_copy(
        src_ref=kv.at[4], dst_ref=kv.at[0], send_sem=ks.at[0], recv_sem=kr.at[0],
        device_id=((ep + 1) % 32, y, x), device_id_type=MESH,
    )
    rim.start()

    l_ow.wait()

    def spread(h, carry):
        w = ow_v[pl.ds(pl.multiple_of(h * HD, HD), HD), :]
        zero = jnp.zeros((HD, 128), bf16)
        w01[pl.ds(pl.multiple_of(h * 128, 128), HD), :] = jnp.concatenate([w, zero], axis=1)
        w01[pl.ds(pl.multiple_of(h * 128 + HD, HD), HD), :] = jnp.concatenate([zero, w], axis=1)
        return carry

    lax.fori_loop(0, HEADS, spread, 0)

    sink = sink_ref[0]
    q_pos = lax.broadcasted_iota(jnp.int32, (WINDOW, 2 * WINDOW), 0) + WINDOW
    k_pos = lax.broadcasted_iota(jnp.int32, (WINDOW, 2 * WINDOW), 1)
    banded = (q_pos >= k_pos) & (q_pos - k_pos < WINDOW)

    def mix_of(n):
        keys = kv[pl.ds(n, 2)].reshape(2 * WINDOW, 128)
        scores = lax.dot_general(qp[n], keys, (((1,), (1,)), ((), ())), preferred_element_type=f32) * HD ** (-0.5)
        allowed = banded & ((ep * 4 + n) * WINDOW + k_pos >= WINDOW)
        scores = jnp.where(allowed, scores, mask_value)
        top = jnp.maximum(jnp.max(scores, axis=1, keepdims=True), sink)
        e = jnp.exp(scores - top)
        total = jnp.sum(e, axis=1, keepdims=True) + jnp.exp(sink - top)
        return dot((e / total).astype(bf16), keys)

    def attend(n):
        mixed = jnp.where(first, pltpu.roll(mix_of(n), HD, 1), mix_of(n + 2)).astype(bf16)
        xg[UNITS + 2 * n, y, x] = mixed[:ROWS].reshape(2, SLOTS, 128)
        xg[UNITS + 2 * n + 1, x, y] = mixed[ROWS:].reshape(2, SLOTS, 128)

    def ag1_copy(u, k):
        i, j = place(u)
        return pltpu.make_async_remote_copy(
            src_ref=xg.at[u, i, j], dst_ref=xg.at[u, i, j],
            send_sem=a1s.at[u, k - 1], recv_sem=a1r.at[u, k - 1],
            device_id=along_j(u, k), device_id_type=MESH,
        )

    def ag3_copy(u, side):
        i, j = place(u)
        return pltpu.make_async_remote_copy(
            src_ref=xg.at[u, i], dst_ref=xg.at[u, i],
            send_sem=a3s.at[u, side], recv_sem=a3r.at[u, side],
            device_id=along_i(u, bw if side else fw), device_id_type=MESH,
        )

    def ag4_copy(u):
        i, j = place(u)
        row = (i + bw) % 4
        return pltpu.make_async_remote_copy(
            src_ref=xg.at[u, row], dst_ref=xg.at[u, row],
            send_sem=a4s.at[u], recv_sem=a4r.at[u],
            device_id=along_i(u, fw), device_id_type=MESH,
        )

    def got(copy_like, dst, sem):
        pltpu.make_async_remote_copy(
            src_ref=dst, dst_ref=dst, send_sem=copy_like, recv_sem=sem,
            device_id=(ep ^ 1, y, x), device_id_type=MESH,
        ).wait_recv()

    def ag1_got(u, k):
        i, j = place(u)
        got(a1s.at[u, k - 1], xg.at[u, i, (j + 4 - k) % 4], a1r.at[u, k - 1])

    def ag3_got(u, side):
        i, j = place(u)
        got(a3s.at[u, side], xg.at[u, (i + (fw if side else bw)) % 4], a3r.at[u, side])

    def ag4_got(u):
        i, j = place(u)
        got(a4s.at[u], xg.at[u, (i + 2) % 4], a4r.at[u])

    def gathered(u):
        odd = u % 2
        tiles = []
        for yy in range(4):
            for xx in range(4):
                a = jnp.where(odd == 1, xx, yy)
                b = jnp.where(odd == 1, yy, xx)
                tiles.append(xg[u, a, b].reshape(ROWS, 128))
        return jnp.concatenate(tiles, axis=1)

    def rs1_copy(u, side):
        i, j = place(u)
        dest = (j + (bw if side else 2)) % 4
        return pltpu.make_async_remote_copy(
            src_ref=yb.at[u, dest], dst_ref=(rb if side else ra).at[u],
            send_sem=b1s.at[u, side], recv_sem=b1r.at[u, side],
            device_id=along_j(u, bw if side else fw), device_id_type=MESH,
        )

    def rs2_copy(u):
        return pltpu.make_async_remote_copy(
            src_ref=tb.at[u], dst_ref=rc.at[u], send_sem=b2s.at[u], recv_sem=b2r.at[u],
            device_id=along_j(u, fw), device_id_type=MESH,
        )

    def rs3_copy(u, k):
        i, j = place(u)
        return pltpu.make_async_remote_copy(
            src_ref=qb.at[u, (i + k) % 4], dst_ref=rd.at[u, k - 1],
            send_sem=b3s.at[u, k - 1], recv_sem=b3r.at[u, k - 1],
            device_id=along_i(u, k), device_id_type=MESH,
        )

    def home_copy(u, cc):
        dest = ((z + unit_dz(u) + NZ) % NZ) * 2 + cc
        return pltpu.make_async_remote_copy(
            src_ref=fb.at[u, cc], dst_ref=home.at[ep],
            send_sem=hs.at[u, cc], recv_sem=hr.at[u, core],
            device_id=(dest, y, x), device_id_type=MESH,
        )

    def not_own(u, cc):
        return jnp.logical_not((u == 9) & (core == cc))

    def tick(t, carry):
        u1 = t

        @pl.when(t == 2)
        def _():
            rim.wait_recv()
            attend(0)

        @pl.when(t == 4)
        def _():
            attend(1)

        @pl.when(u1 < ALL_UNITS)
        def _():
            @pl.when(u1 < UNITS)
            def _():
                for c in (0, 1):
                    @pl.when(not_own(u1, c))
                    def _():
                        z_wait(u1, c)
            for k in (1, 2, 3):
                ag1_copy(u1, k).start()

        u2 = t - RS2

        @pl.when((u2 >= 0) & (u2 < UNITS))
        def _():
            i, j = place(u2)
            rs = rs1_copy(u2, 0)
            rs.wait_recv()
            tb[u2] = (ra[u2].astype(f32) + yb[u2, (j + fw) % 4].astype(f32)).astype(bf16)
            rs2_copy(u2).start()

        u3 = t - AG3

        @pl.when((u3 >= 0) & (u3 < ALL_UNITS))
        def _():
            for k in (1, 2, 3):
                ag1_got(u3, k)
            ag3_copy(u3, 0).start()
            ag3_copy(u3, 1).start()

        u4 = t - AG4

        @pl.when((u4 >= 0) & (u4 < ALL_UNITS))
        def _():
            ag3_got(u4, 0)
            ag4_copy(u4).start()

        u5 = t - RS3

        @pl.when((u5 >= 0) & (u5 < UNITS))
        def _():
            i, j = place(u5)
            rs1_copy(u5, 1).wait_recv()
            rs2_copy(u5).wait_recv()
            qb[u5] = (yb[u5, j].astype(f32) + rc[u5].astype(f32) + rb[u5].astype(f32)).astype(bf16)
            for k in (1, 2, 3):
                rs3_copy(u5, k).start()

        u6 = t - FIN

        @pl.when((u6 >= 0) & (u6 < UNITS))
        def _():
            i, j = place(u6)
            for k in (1, 2, 3):
                rs3_copy(u6, k).wait_recv()
            total = qb[u6, i].astype(f32) + rd[u6, 0].astype(f32) + rd[u6, 1].astype(f32) + rd[u6, 2].astype(f32)
            fb[u6] = total.astype(bf16).reshape(2, SLOTS, 128)
            for cc in (0, 1):
                @pl.when(not_own(u6, cc))
                def _():
                    home_copy(u6, cc).start()

                @pl.when(jnp.logical_not(not_own(u6, cc)))
                def _():
                    home[ep] = fb[u6, cc]

        um = t - MM

        @pl.when(um == 0)
        def _():
            l_wg.wait()
            l_wu.wait()
            l_wd.wait()

        @pl.when((um >= 0) & (um < ALL_UNITS))
        def _():
            ag3_got(um, 1)
            ag4_got(um)

        @pl.when((um >= 0) & (um < UNITS))
        def _():
            i, j = place(um)
            odd = um % 2
            rows_in = gathered(um)
            gate = dot(rows_in, wg_v[...])
            up = dot(rows_in, wu_v[...])
            hidden = (gate / (1.0 + jnp.exp(-gate)) * up).astype(bf16)
            for yy in range(4):
                part = dot(hidden, wd_v[:, yy * 512:(yy + 1) * 512]).astype(bf16)
                for xx in range(4):
                    a = jnp.where(odd == 1, yy, xx)
                    b = jnp.where(odd == 1, xx, yy)
                    yb[um, a, b] = part[:, xx * 128:(xx + 1) * 128]
            rs1_copy(um, 0).start()
            rs1_copy(um, 1).start()

        @pl.when((um >= UNITS) & (um < ALL_UNITS))
        def _():
            out = dot(gathered(um), w01[...]).astype(bf16)
            row = (um - UNITS) * ROWS
            attn_ref[pl.ds(pl.multiple_of(row, ROWS), ROWS), :] = out[:, :128]
            attn_ref[pl.ds(pl.multiple_of(row + 256, ROWS), ROWS), :] = out[:, 128:]

        @pl.when((u6 >= 0) & (u6 < ALL_UNITS))
        def _():
            for k in (1, 2, 3):
                ag1_copy(u6, k).wait_send()
            ag3_copy(u6, 0).wait_send()
            ag3_copy(u6, 1).wait_send()
            ag4_copy(u6).wait_send()

        @pl.when((u6 >= 0) & (u6 < UNITS))
        def _():
            for cc in (0, 1):
                @pl.when(not_own(u6, cc))
                def _():
                    z_copy(u6, cc).wait_send()
            rs1_copy(u6, 0).wait_send()
            rs1_copy(u6, 1).wait_send()
            rs2_copy(u6).wait_send()
            for k in (1, 2, 3):
                rs3_copy(u6, k).wait_send()

        return carry

    lax.fori_loop(0, ALL_UNITS + FIN, tick, 0)

    l_rw.wait()
    weights = rw_v[...]
    slot0 = jnp.sum(one0 * (rank + e_iota.astype(f32) * float(SLOTS)), axis=1, keepdims=True)
    slot1 = jnp.sum(one1 * (rank + e_iota.astype(f32) * float(SLOTS)), axis=1, keepdims=True)
    slot_lane = lax.broadcasted_iota(jnp.int32, (TOK_E, EXPERTS * SLOTS), 1).astype(f32)
    pick0 = (slot_lane == slot0).astype(f32).astype(bf16)
    pick1 = (slot_lane == slot1).astype(f32).astype(bf16)

    def arrived(u, carry):
        for c in (0, 1):
            @pl.when(not_own(u, c))
            def _():
                src = ((z - unit_dz(u) + NZ) % NZ) * 2 + c
                got(hs.at[u, c], home.at[src], hr.at[u, c])
                home_copy(u, c).wait_send()
        return carry

    lax.fori_loop(0, UNITS, arrived, 0)
    rim.wait_send()
    results = home[...].reshape(EXPERTS * SLOTS, 128)
    combined = dot(pick0, results) * weights[:, 0:1] + dot(pick1, results) * weights[:, 1:2]
    eout_ref[...] = combined.astype(bf16)


def local(
    queries,
    keys,
    values,
    sink_logits,
    out_weight,
    expert_input,
    norm_gain,
    routes,
    route_weights,
    gate_weight,
    up_weight,
    down_weight,
):
    any_spec = pl.BlockSpec(memory_space=pl.ANY)
    vmem = pl.BlockSpec(memory_space=pltpu.VMEM)
    smem = pl.BlockSpec(memory_space=pltpu.SMEM)
    dma = pltpu.SemaphoreType.DMA
    trig = jnp.asarray(rope_tables())
    return pl.pallas_call(
        kernel,
        out_shape=(
            jax.ShapeDtypeStruct((TOK_A, 128), bf16),
            jax.ShapeDtypeStruct((TOK_E, 128), bf16),
        ),
        in_specs=[any_spec] * 3 + [smem] + [any_spec] * 9,
        out_specs=(vmem, vmem),
        scratch_shapes=[
            pltpu.VMEM((TOK_A, HD), bf16),
            pltpu.VMEM((TOK_A, 128), bf16),
            pltpu.VMEM((TOK_A, 128), bf16),
            pltpu.VMEM((HEADS * HD, 128), bf16),
            pltpu.VMEM((TOK_E, D), bf16),
            pltpu.VMEM((1, D), f32),
            pltpu.VMEM((TOK_E, 2), jnp.int32),
            pltpu.VMEM((TOK_E, 2), f32),
            pltpu.VMEM((D, FF_HERE), bf16),
            pltpu.VMEM((D, FF_HERE), bf16),
            pltpu.VMEM((FF_HERE, D), bf16),
            pltpu.VMEM((4, 128, 128), f32),
            pltpu.VMEM((TOK_E, 128), bf16),
            pltpu.VMEM((EXPERTS, SLOTS, 128), bf16),
            pltpu.VMEM((D, 256), bf16),
            pltpu.VMEM((4, WINDOW, 128), bf16),
            pltpu.VMEM((5, WINDOW, 128), bf16),
            pltpu.VMEM((ALL_UNITS, 4, 4, 2, SLOTS, 128), bf16),
            pltpu.VMEM((UNITS, 4, 4, ROWS, 128), bf16),
            pltpu.VMEM((UNITS, 4, ROWS, 128), bf16),
            pltpu.VMEM((UNITS, 4, ROWS, 128), bf16),
            pltpu.VMEM((UNITS, 4, ROWS, 128), bf16),
            pltpu.VMEM((UNITS, 4, ROWS, 128), bf16),
            pltpu.VMEM((UNITS, 4, ROWS, 128), bf16),
            pltpu.VMEM((UNITS, 3, ROWS, 128), bf16),
            pltpu.VMEM((UNITS, 2, SLOTS, 128), bf16),
            pltpu.VMEM((EXPERTS, SLOTS, 128), bf16),
            dma((12,)),
            dma((UNITS, 2)),
            dma((UNITS, 2)),
            dma((UNITS, 2)),
            dma((UNITS, 2)),
            dma((ALL_UNITS, 3)),
            dma((ALL_UNITS, 3)),
            dma((ALL_UNITS, 2)),
            dma((ALL_UNITS, 2)),
            dma((ALL_UNITS,)),
            dma((ALL_UNITS,)),
            dma((UNITS, 2)),
            dma((UNITS, 2)),
            dma((UNITS,)),
            dma((UNITS,)),
            dma((UNITS, 3)),
            dma((UNITS, 3)),
            dma((1,)),
            dma((1,)),
        ],
        compiler_params=pltpu.CompilerParams(
            collective_id=0, has_side_effects=True, vmem_limit_bytes=60 * 1024 * 1024
        ),
    )(
        queries, keys, values, sink_logits, out_weight, expert_input, norm_gain.reshape(1, D), routes, route_weights,
        gate_weight[0], up_weight[0], down_weight[0], trig,
    )


def solution(mesh):
    finer = Mesh(mesh.devices.reshape(mesh.shape["ep"], 4, 4), ("ep", "tp_0", "tp_1"))
    return jax.shard_map(
        local,
        mesh=finer,
        in_specs=(
            P("ep", TP),
            P("ep", None),
            P("ep", None),
            P(TP),
            P(None, TP),
            P("ep", None),
            P(),
            P("ep", None),
            P("ep", None),
            P("ep", None, TP),
            P("ep", None, TP),
            P("ep", TP, None),
        ),
        out_specs=(P("ep", TP), P("ep", TP)),
        check_vma=False,
    )
```

```python
import jax
import jax.numpy as jnp
import numpy as np
from jax import lax
from jax.experimental import pallas as pl
from jax.experimental.pallas import tpu as pltpu
from jax.sharding import Mesh
from jax.sharding import PartitionSpec as P

HEADS = 16
KV = 2
HD = 64
WINDOW = 128
TP = ("tp_0", "tp_1")
NZ = 16
UNITS = 16
ATT_UNITS = 4
ALL_UNITS = UNITS + ATT_UNITS
SLOTS = 32
EXPERTS = 32
ROWS = 64
D = 2048
FF_HERE = 256
TOK_E = 256
TOK_A = 512
MESH = pl.DeviceIdType.MESH
OWN = 15
ATTEND = (8, 10)

AG3, AG4, MM, RS2, RS3, FIN = 2, 4, 6, 8, 10, 12

rms_eps = 1e-06
mask_value = -1e30

f32 = jnp.float32
bf16 = jnp.bfloat16


def unit_dz(u):
    late = u - 7
    out = jnp.where(u == 6, 8, (2 + 2 * (u // 2)) * (1 - 2 * (u % 2)))
    back = jnp.where(u == OWN, 0, (7 - 2 * (late // 2)) * (1 - 2 * (late % 2)))
    return jnp.where(u < 7, out, back)


def rope_tables():
    lane = np.arange(128) % 32
    freq = 10000.0 ** (-lane * (2.0 / HD))
    sign = np.where(np.arange(128) % 64 < 32, -1.0, 1.0)
    near = np.arange(WINDOW)[:, None] * freq[None, :]
    far = (np.arange(128) * WINDOW)[:, None] * freq[None, :]
    tables = np.stack([np.cos(near), np.sin(near) * sign, np.cos(far), np.sin(far) * sign])
    return tables.astype(np.float32)


def dot(a, b):
    return jnp.dot(a, b, preferred_element_type=f32)


def kernel(
    q_in, k_in, v_in, sink_ref, ow_in, x_in, gain_in, routes_in, rw_in, wg_in, wu_in, wd_in, trig_in,
    attn_ref, eout_ref,
    q_v, k_v, v_v, ow_v, x_v, gain_v, routes_v, rw_v, wg_v, wu_v, wd_v, trig_v,
    nrm, disp, w01, qp, kv, xg, yb, ra, rb, rc, tb, qb, rd, fb, home,
    in_sem, zs, zr, hs, hr, ags, a1r, a3r, a4r, rss, b1r, b2r, b3r, rims, rimr,
):
    ep = lax.axis_index("ep")
    y = lax.axis_index("tp_0")
    x = lax.axis_index("tp_1")
    z = ep // 2
    core = ep % 2
    tp = y * 4 + x
    sg = 1 - 2 * core

    pairs = [
        (routes_in, routes_v), (x_in, x_v), (gain_in, gain_v), (rw_in, rw_v), (trig_in, trig_v), (q_in, q_v),
        (k_in, k_v), (v_in, v_v), (wg_in, wg_v), (wu_in, wu_v), (wd_in, wd_v), (ow_in, ow_v),
    ]
    loads = [pltpu.make_async_copy(a, b, in_sem.at[n]) for n, (a, b) in enumerate(pairs)]
    for load in loads:
        load.start()
    (l_routes, l_x, l_gain, l_rw, l_trig, l_q, l_k, l_v, l_wg, l_wu, l_wd, l_ow) = loads

    barrier = pltpu.get_barrier_semaphore()

    def hello(step, carry):
        pl.semaphore_signal(barrier, inc=1, device_id=((ep + step) % 32, y, x), device_id_type=MESH)
        return carry

    lax.fori_loop(1, 32, hello, 0)
    for k in (1, 2, 3):
        pl.semaphore_signal(barrier, inc=1, device_id=(ep, (y + k) % 4, x), device_id_type=MESH)
        pl.semaphore_signal(barrier, inc=1, device_id=(ep, y, (x + k) % 4), device_id_type=MESH)

    l_routes.wait()
    e_iota = lax.broadcasted_iota(jnp.int32, (EXPERTS, TOK_E), 0)
    one0 = (routes_v[0:1, :] == e_iota).astype(f32)
    one1 = (routes_v[1:2, :] == e_iota).astype(f32)
    t_row = lax.broadcasted_iota(jnp.int32, (TOK_E, TOK_E), 0)
    t_col = lax.broadcasted_iota(jnp.int32, (TOK_E, TOK_E), 1)
    before = (t_row < t_col).astype(f32).astype(bf16)
    place_of = dot((one0 + one1).astype(bf16), before) + (e_iota * SLOTS).astype(f32)
    slot_row0 = jnp.sum(one0 * place_of, axis=0, keepdims=True)
    slot_row1 = jnp.sum(one1 * place_of, axis=0, keepdims=True)

    l_x.wait()
    l_gain.wait()
    own_cols = pl.ds(pl.multiple_of(tp * 128, 128), 128)
    gain = gain_v[:, own_cols]

    def norm_rows(n, carry):
        rows = pl.ds(pl.multiple_of(n * 32, 32), 32)
        wide = x_v[rows, :].astype(f32)
        inv = lax.rsqrt(jnp.mean(wide * wide, axis=1, keepdims=True) + rms_eps)
        nrm[rows, :] = (x_v[rows, own_cols].astype(f32) * inv * gain).astype(bf16)
        return carry

    lax.fori_loop(0, 8, norm_rows, 0)
    normed = nrm[...]

    def fill_slots(n, carry):
        slot = (lax.broadcasted_iota(jnp.int32, (256, TOK_E), 0) + n * 256).astype(f32)
        pick = ((slot == slot_row0) | (slot == slot_row1)).astype(f32).astype(bf16)
        disp[pl.ds(n * 8, 8)] = dot(pick, normed).astype(bf16).reshape(8, SLOTS, 128)
        return carry

    lax.fori_loop(0, 4, fill_slots, 0)
    pl.semaphore_wait(barrier, 37)

    def place(u):
        odd = u % 2
        return jnp.where(odd == 1, x, y), jnp.where(odd == 1, y, x)

    def along_j(u, k):
        odd = u % 2
        return (ep, jnp.where(odd == 1, (y + k) % 4, y), jnp.where(odd == 1, x, (x + k) % 4))

    def along_i(u, k):
        odd = u % 2
        return (ep, jnp.where(odd == 1, y, (y + k) % 4), jnp.where(odd == 1, (x + k) % 4, x))

    fw = sg + 4
    bw = 4 - sg

    def got(like, sem):
        pltpu.make_async_remote_copy(
            src_ref=like, dst_ref=like, send_sem=rims.at[0], recv_sem=sem,
            device_id=(ep ^ 1, y, x), device_id_type=MESH,
        ).wait_recv()

    def left(like, sem):
        pltpu.make_async_remote_copy(
            src_ref=like, dst_ref=like, send_sem=sem, recv_sem=rimr.at[0],
            device_id=(ep ^ 1, y, x), device_id_type=MESH,
        ).wait_send()

    def z_copy(u, cc):
        dest = ((z - unit_dz(u) + NZ) % NZ) * 2 + cc
        i, j = place(u)
        return pltpu.make_async_remote_copy(
            src_ref=disp.at[dest], dst_ref=xg.at[u, 4 * i + j, core],
            send_sem=zs.at[0], recv_sem=zr.at[u],
            device_id=(dest, y, x), device_id_type=MESH,
        )

    def z_wait(u):
        i, j = place(u)

        @pl.when(u != OWN)
        def _():
            got(xg.at[u, 4 * i + j], zr.at[u])

        @pl.when(u == OWN)
        def _():
            got(xg.at[u, 4 * i + j, 1 - core], zr.at[u])

    def z_send(u, carry):
        for cc in (0, 1):
            @pl.when(jnp.logical_not((u == OWN) & (core == cc)))
            def _():
                z_copy(u, cc).start()
        return carry

    lax.fori_loop(0, UNITS, z_send, 0)
    xg[OWN, 4 * x + y, core] = disp[ep]

    l_trig.wait()
    l_q.wait()
    l_k.wait()
    l_v.wait()
    group = y // 2
    lane = lax.broadcasted_iota(jnp.int32, (WINDOW, 128), 1)
    first = lane < HD

    def rotate_block(n, carry):
        rows = pl.ds(pl.multiple_of(n * WINDOW, WINDOW), WINDOW)
        q = q_v[:, rows].astype(f32)
        k = k_v[rows, :].astype(f32)
        v = v_v[rows, :].astype(f32)
        k = jnp.where(group == 0, pltpu.roll(k, HD, 1), k)
        v = jnp.where(group == 0, pltpu.roll(v, HD, 1), v)
        both = jnp.where(first, jnp.concatenate([q, q], axis=0).T, k)
        block = ep * 4 + n
        cb = trig_v[2, pl.ds(block, 1), :]
        sb = trig_v[3, pl.ds(block, 1), :]
        cr = trig_v[0]
        sr = trig_v[1]
        cos = cb * cr - sb * sr
        sin = sb * cr + cb * sr
        swapped = jnp.where(lane % HD < HD // 2, pltpu.roll(both, 128 - HD // 2, 1), pltpu.roll(both, HD // 2, 1))
        turned = both * cos + swapped * sin
        qp[n] = jnp.where(first, turned, 0.0).astype(bf16)
        kv[n + 1] = jnp.where(first, pltpu.roll(turned, HD, 1), v).astype(bf16)
        return carry

    lax.fori_loop(0, 4, rotate_block, 0)
    rim = pltpu.make_async_remote_copy(
        src_ref=kv.at[4], dst_ref=kv.at[0], send_sem=rims.at[0], recv_sem=rimr.at[0],
        device_id=((ep + 1) % 32, y, x), device_id_type=MESH,
    )
    rim.start()

    l_ow.wait()

    def spread(h, carry):
        w = ow_v[pl.ds(pl.multiple_of(h * HD, HD), HD), :]
        zero = jnp.zeros((HD, 128), bf16)
        w01[pl.ds(pl.multiple_of(h * 128, 128), HD), :] = jnp.concatenate([w, zero], axis=1)
        w01[pl.ds(pl.multiple_of(h * 128 + HD, HD), HD), :] = jnp.concatenate([zero, w], axis=1)
        return carry

    lax.fori_loop(0, HEADS, spread, 0)

    sink = sink_ref[0]
    q_pos = lax.broadcasted_iota(jnp.int32, (WINDOW, 2 * WINDOW), 0) + WINDOW
    k_pos = lax.broadcasted_iota(jnp.int32, (WINDOW, 2 * WINDOW), 1)
    banded = (q_pos >= k_pos) & (q_pos - k_pos < WINDOW)

    def mix_of(n):
        keys = kv[pl.ds(n, 2)].reshape(2 * WINDOW, 128)
        scores = lax.dot_general(qp[n], keys, (((1,), (1,)), ((), ())), preferred_element_type=f32) * HD ** (-0.5)
        allowed = banded & ((ep * 4 + n) * WINDOW + k_pos >= WINDOW)
        scores = jnp.where(allowed, scores, mask_value)
        top = jnp.maximum(jnp.max(scores, axis=1, keepdims=True), sink)
        e = jnp.exp(scores - top)
        total = jnp.sum(e, axis=1, keepdims=True) + jnp.exp(sink - top)
        return dot((e / total).astype(bf16), keys)

    def attend(n):
        mixed = jnp.where(first, pltpu.roll(mix_of(n), HD, 1), mix_of(n + 2)).astype(bf16)
        xg[UNITS + 2 * n, 4 * y + x] = mixed[:ROWS].reshape(2, SLOTS, 128)
        xg[UNITS + 2 * n + 1, 4 * x + y] = mixed[ROWS:].reshape(2, SLOTS, 128)

    def ag1_copy(u, k):
        i, j = place(u)
        return pltpu.make_async_remote_copy(
            src_ref=xg.at[u, 4 * i + j], dst_ref=xg.at[u, 4 * i + j],
            send_sem=ags.at[u], recv_sem=a1r.at[u],
            device_id=along_j(u, k), device_id_type=MESH,
        )

    def ag3_copy(u, side):
        i, j = place(u)
        return pltpu.make_async_remote_copy(
            src_ref=xg.at[u, pl.ds(4 * i, 4)], dst_ref=xg.at[u, pl.ds(4 * i, 4)],
            send_sem=ags.at[u], recv_sem=(a4r if side else a3r).at[u],
            device_id=along_i(u, bw if side else fw), device_id_type=MESH,
        )

    def ag4_copy(u):
        i, j = place(u)
        row = (i + bw) % 4
        return pltpu.make_async_remote_copy(
            src_ref=xg.at[u, pl.ds(4 * row, 4)], dst_ref=xg.at[u, pl.ds(4 * row, 4)],
            send_sem=ags.at[u], recv_sem=a4r.at[u],
            device_id=along_i(u, fw), device_id_type=MESH,
        )

    def gathered(u):
        odd = u % 2
        tiles = []
        for yy in range(4):
            for xx in range(4):
                a = jnp.where(odd == 1, xx, yy)
                b = jnp.where(odd == 1, yy, xx)
                tiles.append(xg[u, 4 * a + b].reshape(ROWS, 128))
        return jnp.concatenate(tiles, axis=1)

    def rs1_copy(u, side):
        i, j = place(u)
        dest = (j + (bw if side else 2)) % 4
        return pltpu.make_async_remote_copy(
            src_ref=yb.at[u, dest], dst_ref=(rb if side else ra).at[u],
            send_sem=rss.at[u], recv_sem=(b2r if side else b1r).at[u],
            device_id=along_j(u, bw if side else fw), device_id_type=MESH,
        )

    def rs2_copy(u):
        return pltpu.make_async_remote_copy(
            src_ref=tb.at[u], dst_ref=rc.at[u], send_sem=rss.at[u], recv_sem=b2r.at[u],
            device_id=along_j(u, fw), device_id_type=MESH,
        )

    def rs3_copy(u, k):
        i, j = place(u)
        return pltpu.make_async_remote_copy(
            src_ref=qb.at[u, (i + k) % 4], dst_ref=rd.at[u, k - 1],
            send_sem=rss.at[u], recv_sem=b3r.at[u],
            device_id=along_i(u, k), device_id_type=MESH,
        )

    def home_copy(u, cc):
        dest = ((z + unit_dz(u) + NZ) % NZ) * 2 + cc
        return pltpu.make_async_remote_copy(
            src_ref=fb.at[u, cc], dst_ref=home.at[ep],
            send_sem=hs.at[0], recv_sem=hr.at[0],
            device_id=(dest, y, x), device_id_type=MESH,
        )

    def not_own(u, cc):
        return jnp.logical_not((u == OWN) & (core == cc))

    def tick(t, carry):
        u1 = t

        @pl.when(t == ATTEND[0])
        def _():
            rim.wait_recv()
            attend(0)

        @pl.when(t == ATTEND[1])
        def _():
            attend(1)

        @pl.when(u1 < ALL_UNITS)
        def _():
            @pl.when(u1 < UNITS)
            def _():
                z_wait(u1)
            for k in (1, 2, 3):
                ag1_copy(u1, k).start()

        u2 = t - RS2

        @pl.when((u2 >= 0) & (u2 < UNITS))
        def _():
            i, j = place(u2)
            got(ra.at[u2], b1r.at[u2])
            tb[u2] = (ra[u2].astype(f32) + yb[u2, (j + fw) % 4].astype(f32)).astype(bf16)
            rs2_copy(u2).start()

        u3 = t - AG3

        @pl.when((u3 >= 0) & (u3 < ALL_UNITS))
        def _():
            got(xg.at[u3, pl.ds(0, 3)], a1r.at[u3])
            ag3_copy(u3, 0).start()
            ag3_copy(u3, 1).start()

        u4 = t - AG4

        @pl.when((u4 >= 0) & (u4 < ALL_UNITS))
        def _():
            got(xg.at[u4, pl.ds(0, 4)], a3r.at[u4])
            ag4_copy(u4).start()

        u5 = t - RS3

        @pl.when((u5 >= 0) & (u5 < UNITS))
        def _():
            i, j = place(u5)
            got(xg.at[u5, pl.ds(0, 8)], b2r.at[u5])
            qb[u5] = (yb[u5, j].astype(f32) + rc[u5].astype(f32) + rb[u5].astype(f32)).astype(bf16)
            for k in (1, 2, 3):
                rs3_copy(u5, k).start()

        u6 = t - FIN

        @pl.when((u6 >= 0) & (u6 < UNITS))
        def _():
            i, j = place(u6)
            got(rd.at[u6], b3r.at[u6])
            total = qb[u6, i].astype(f32) + rd[u6, 0].astype(f32) + rd[u6, 1].astype(f32) + rd[u6, 2].astype(f32)
            fb[u6] = total.astype(bf16).reshape(2, SLOTS, 128)
            for cc in (0, 1):
                @pl.when(not_own(u6, cc))
                def _():
                    home_copy(u6, cc).start()

                @pl.when(jnp.logical_not(not_own(u6, cc)))
                def _():
                    home[ep] = fb[u6, cc]

        um = t - MM

        @pl.when(um == 0)
        def _():
            l_wg.wait()
            l_wu.wait()
            l_wd.wait()

        @pl.when((um >= 0) & (um < ALL_UNITS))
        def _():
            got(xg.at[um, pl.ds(0, 8)], a4r.at[um])

        @pl.when((um >= 0) & (um < UNITS))
        def _():
            i, j = place(um)
            odd = um % 2
            rows_in = gathered(um)
            gate = dot(rows_in, wg_v[...])
            up = dot(rows_in, wu_v[...])
            hidden = (gate / (1.0 + jnp.exp(-gate)) * up).astype(bf16)
            for yy in range(4):
                part = dot(hidden, wd_v[:, yy * 512:(yy + 1) * 512]).astype(bf16)
                for xx in range(4):
                    a = jnp.where(odd == 1, yy, xx)
                    b = jnp.where(odd == 1, xx, yy)
                    yb[um, a, b] = part[:, xx * 128:(xx + 1) * 128]
            rs1_copy(um, 0).start()
            rs1_copy(um, 1).start()

        @pl.when((um >= UNITS) & (um < ALL_UNITS))
        def _():
            out = dot(gathered(um), w01[...]).astype(bf16)
            row = (um - UNITS) * ROWS
            attn_ref[pl.ds(pl.multiple_of(row, ROWS), ROWS), :] = out[:, :128]
            attn_ref[pl.ds(pl.multiple_of(row + 256, ROWS), ROWS), :] = out[:, 128:]

        @pl.when((u6 >= 0) & (u6 < ALL_UNITS))
        def _():
            left(xg.at[u6, pl.ds(0, 15)], ags.at[u6])

        @pl.when((u6 >= 0) & (u6 < UNITS))
        def _():
            left(xg.at[u6, pl.ds(0, 15)], rss.at[u6])

        return carry

    lax.fori_loop(0, ALL_UNITS + FIN, tick, 0)

    l_rw.wait()
    eye = t_col == t_row

    def as_column(row):
        return jnp.sum(jnp.where(eye, row, 0.0), axis=1, keepdims=True)

    weight0 = as_column(rw_v[0:1, :])
    weight1 = as_column(rw_v[1:2, :])
    slot0 = as_column(slot_row0)
    slot1 = as_column(slot_row1)
    slot_lane = lax.broadcasted_iota(jnp.int32, (TOK_E, EXPERTS * SLOTS), 1).astype(f32)
    pick0 = (slot_lane == slot0).astype(f32).astype(bf16)
    pick1 = (slot_lane == slot1).astype(f32).astype(bf16)

    got(home.at[pl.ds(0, EXPERTS - 1)], hr.at[0])
    left(home.at[pl.ds(0, EXPERTS - 1)], hs.at[0])
    left(disp.at[pl.ds(0, EXPERTS - 1)], zs.at[0])
    rim.wait_send()
    results = home[...].reshape(EXPERTS * SLOTS, 128)
    combined = dot(pick0, results) * weight0 + dot(pick1, results) * weight1
    eout_ref[...] = combined.astype(bf16)


def local(
    queries,
    keys,
    values,
    sink_logits,
    out_weight,
    expert_input,
    norm_gain,
    routes,
    route_weights,
    gate_weight,
    up_weight,
    down_weight,
):
    any_spec = pl.BlockSpec(memory_space=pl.ANY)
    vmem = pl.BlockSpec(memory_space=pltpu.VMEM)
    smem = pl.BlockSpec(memory_space=pltpu.SMEM)
    dma = pltpu.SemaphoreType.DMA
    trig = jnp.asarray(rope_tables())
    return pl.pallas_call(
        kernel,
        out_shape=(
            jax.ShapeDtypeStruct((TOK_A, 128), bf16),
            jax.ShapeDtypeStruct((TOK_E, 128), bf16),
        ),
        in_specs=[any_spec] * 3 + [smem] + [any_spec] * 9,
        out_specs=(vmem, vmem),
        scratch_shapes=[
            pltpu.VMEM((HD, TOK_A), bf16),
            pltpu.VMEM((TOK_A, 128), bf16),
            pltpu.VMEM((TOK_A, 128), bf16),
            pltpu.VMEM((HEADS * HD, 128), bf16),
            pltpu.VMEM((TOK_E, D), bf16),
            pltpu.VMEM((1, D), f32),
            pltpu.VMEM((2, TOK_E), jnp.int32),
            pltpu.VMEM((2, TOK_E), f32),
            pltpu.VMEM((D, FF_HERE), bf16),
            pltpu.VMEM((D, FF_HERE), bf16),
            pltpu.VMEM((FF_HERE, D), bf16),
            pltpu.VMEM((4, 128, 128), f32),
            pltpu.VMEM((TOK_E, 128), bf16),
            pltpu.VMEM((EXPERTS, SLOTS, 128), bf16),
            pltpu.VMEM((D, 256), bf16),
            pltpu.VMEM((4, WINDOW, 128), bf16),
            pltpu.VMEM((5, WINDOW, 128), bf16),
            pltpu.VMEM((ALL_UNITS, 16, 2, SLOTS, 128), bf16),
            pltpu.VMEM((UNITS, 4, 4, ROWS, 128), bf16),
            pltpu.VMEM((UNITS, 4, ROWS, 128), bf16),
            pltpu.VMEM((UNITS, 4, ROWS, 128), bf16),
            pltpu.VMEM((UNITS, 4, ROWS, 128), bf16),
            pltpu.VMEM((UNITS, 4, ROWS, 128), bf16),
            pltpu.VMEM((UNITS, 4, ROWS, 128), bf16),
            pltpu.VMEM((UNITS, 3, ROWS, 128), bf16),
            pltpu.VMEM((UNITS, 2, SLOTS, 128), bf16),
            pltpu.VMEM((EXPERTS, SLOTS, 128), bf16),
            dma((12,)),
            dma((1,)),
            dma((UNITS,)),
            dma((1,)),
            dma((1,)),
            dma((ALL_UNITS,)),
            dma((ALL_UNITS,)),
            dma((ALL_UNITS,)),
            dma((ALL_UNITS,)),
            dma((UNITS,)),
            dma((UNITS,)),
            dma((UNITS,)),
            dma((UNITS,)),
            dma((1,)),
            dma((1,)),
        ],
        compiler_params=pltpu.CompilerParams(
            collective_id=0, has_side_effects=True, vmem_limit_bytes=60 * 1024 * 1024
        ),
    )(
        queries.T, keys, values, sink_logits, out_weight, expert_input, norm_gain.reshape(1, D), routes.T, route_weights.T,
        gate_weight[0], up_weight[0], down_weight[0], trig,
    )


def solution(mesh):
    finer = Mesh(mesh.devices.reshape(mesh.shape["ep"], 4, 4), ("ep", "tp_0", "tp_1"))
    return jax.shard_map(
        local,
        mesh=finer,
        in_specs=(
            P("ep", TP),
            P("ep", None),
            P("ep", None),
            P(TP),
            P(None, TP),
            P("ep", None),
            P(),
            P("ep", None),
            P("ep", None),
            P("ep", None, TP),
            P("ep", None, TP),
            P("ep", TP, None),
        ),
        out_specs=(P("ep", TP), P("ep", TP)),
        check_vma=False,
    )
```

```python
import jax
import jax.numpy as jnp
import numpy as np
from jax import lax
from jax.experimental import pallas as pl
from jax.experimental.pallas import tpu as pltpu
from jax.sharding import Mesh
from jax.sharding import PartitionSpec as P

HEADS = 16
KV = 2
HD = 64
WINDOW = 128
TP = ("tp_0", "tp_1")
NZ = 16
UNITS = 16
ATT_UNITS = 4
ALL_UNITS = UNITS + ATT_UNITS
SLOTS = 32
EXPERTS = 32
ROWS = 64
D = 2048
FF_HERE = 256
TOK_E = 256
TOK_A = 512
MESH = pl.DeviceIdType.MESH
OWN = 15
LEAD = 5
ATTEND = (8, 10)

AG3, AG4, MM, RS2, RS3, FIN = 3, 6, 9, 12, 15, 18

rms_eps = 1e-06
mask_value = -1e30

f32 = jnp.float32
bf16 = jnp.bfloat16


def unit_dz(u):
    sign = 1 - 2 * (u % 2)
    out = jnp.where(u == 10, 8, (2 + u // 2) * sign)
    back = jnp.where(u == OWN, 0, jnp.where(u < 13, -7 * sign, -1 * sign))
    return jnp.where(u < 11, out, back)


def rope_tables():
    lane = np.arange(128) % 32
    freq = 10000.0 ** (-lane * (2.0 / HD))
    sign = np.where(np.arange(128) % 64 < 32, -1.0, 1.0)
    near = np.arange(WINDOW)[:, None] * freq[None, :]
    far = (np.arange(128) * WINDOW)[:, None] * freq[None, :]
    tables = np.stack([np.cos(near), np.sin(near) * sign, np.cos(far), np.sin(far) * sign])
    return tables.astype(np.float32)


def dot(a, b):
    return jnp.dot(a, b, preferred_element_type=f32)


def kernel(
    q_in, k_in, v_in, sink_ref, ow_in, x_in, gain_in, routes_in, rw_in, wg_in, wu_in, wd_in, trig_in,
    attn_ref, eout_ref,
    q_v, k_v, v_v, ow_v, x_v, gain_v, routes_v, rw_v, wg_v, wu_v, wd_v, trig_v,
    disp, w01, qp, kv, xg, yb, ra, rb, rc, tb, qb, rd, fb, home,
    in_sem, zs, zr, hs, hr, ags, a1r, a3r, a4r, rss, b1r, b2r, b3r, rims, rimr,
):
    ep = lax.axis_index("ep")
    y = lax.axis_index("tp_0")
    x = lax.axis_index("tp_1")
    z = ep // 2
    core = ep % 2
    tp = y * 4 + x
    sg = 1 - 2 * core

    barrier = pltpu.get_barrier_semaphore()

    for step in sorted(range(1, 32), key=lambda n: -min(n, 32 - n)):
        pl.semaphore_signal(barrier, inc=1, device_id=((ep + step) % 32, y, x), device_id_type=MESH)
    for k in (1, 2, 3):
        pl.semaphore_signal(barrier, inc=1, device_id=(ep, (y + k) % 4, x), device_id_type=MESH)
        pl.semaphore_signal(barrier, inc=1, device_id=(ep, y, (x + k) % 4), device_id_type=MESH)

    pairs = [
        (routes_in, routes_v), (x_in, x_v), (gain_in, gain_v), (rw_in, rw_v), (trig_in, trig_v), (q_in, q_v),
        (k_in, k_v), (v_in, v_v), (wg_in, wg_v), (wu_in, wu_v), (wd_in, wd_v), (ow_in, ow_v),
    ]
    loads = [pltpu.make_async_copy(a, b, in_sem.at[n]) for n, (a, b) in enumerate(pairs)]
    for load in loads:
        load.start()
    (l_routes, l_x, l_gain, l_rw, l_trig, l_q, l_k, l_v, l_wg, l_wu, l_wd, l_ow) = loads

    l_routes.wait()
    e_iota = lax.broadcasted_iota(jnp.int32, (EXPERTS, TOK_E), 0)
    one0 = (routes_v[0:1, :] == e_iota).astype(f32)
    one1 = (routes_v[1:2, :] == e_iota).astype(f32)
    t_row = lax.broadcasted_iota(jnp.int32, (TOK_E, TOK_E), 0)
    t_col = lax.broadcasted_iota(jnp.int32, (TOK_E, TOK_E), 1)
    before = (t_row < t_col).astype(f32).astype(bf16)
    place_of = dot((one0 + one1).astype(bf16), before) + (e_iota * SLOTS).astype(f32)
    slot_row0 = jnp.sum(one0 * place_of, axis=0, keepdims=True)
    slot_row1 = jnp.sum(one1 * place_of, axis=0, keepdims=True)

    l_x.wait()
    l_gain.wait()
    own_cols = pl.ds(pl.multiple_of(tp * 128, 128), 128)
    gain = gain_v[:, own_cols]

    squares = jnp.zeros((TOK_E, 128), f32)
    for n in range(D // 128):
        wide = x_v[:, n * 128:(n + 1) * 128].astype(f32)
        squares = squares + wide * wide
    inv = lax.rsqrt(jnp.sum(squares, axis=1, keepdims=True) * (1.0 / D) + rms_eps)
    normed = (x_v[:, own_cols].astype(f32) * inv * gain).astype(bf16)

    def fill_slots(n, carry):
        slot = (lax.broadcasted_iota(jnp.int32, (256, TOK_E), 0) + n * 256).astype(f32)
        pick = ((slot == slot_row0) | (slot == slot_row1)).astype(f32).astype(bf16)
        disp[pl.ds(n * 8, 8)] = dot(pick, normed).astype(bf16).reshape(8, SLOTS, 128)
        return carry

    lax.fori_loop(0, 4, fill_slots, 0)
    pl.semaphore_wait(barrier, 37)

    def place(u):
        odd = u % 2
        return jnp.where(odd == 1, x, y), jnp.where(odd == 1, y, x)

    def along_j(u, k):
        odd = u % 2
        return (ep, jnp.where(odd == 1, (y + k) % 4, y), jnp.where(odd == 1, x, (x + k) % 4))

    def along_i(u, k):
        odd = u % 2
        return (ep, jnp.where(odd == 1, y, (y + k) % 4), jnp.where(odd == 1, (x + k) % 4, x))

    fw = sg + 4
    bw = 4 - sg

    def got(like, sem):
        pltpu.make_async_remote_copy(
            src_ref=like, dst_ref=like, send_sem=rims.at[0], recv_sem=sem,
            device_id=(ep ^ 1, y, x), device_id_type=MESH,
        ).wait_recv()

    def left(like, sem):
        pltpu.make_async_remote_copy(
            src_ref=like, dst_ref=like, send_sem=sem, recv_sem=rimr.at[0],
            device_id=(ep ^ 1, y, x), device_id_type=MESH,
        ).wait_send()

    def z_copy(u, cc):
        dest = ((z - unit_dz(u) + NZ) % NZ) * 2 + cc
        i, j = place(u)
        return pltpu.make_async_remote_copy(
            src_ref=disp.at[dest], dst_ref=xg.at[u, 4 * i + j, core],
            send_sem=zs.at[0], recv_sem=zr.at[u],
            device_id=(dest, y, x), device_id_type=MESH,
        )

    def z_wait(u):
        i, j = place(u)

        @pl.when(u != OWN)
        def _():
            got(xg.at[u, 4 * i + j], zr.at[u])

        @pl.when(u == OWN)
        def _():
            got(xg.at[u, 4 * i + j, 1 - core], zr.at[u])

    def z_send(u, carry):
        for cc in (0, 1):
            @pl.when(jnp.logical_not((u == OWN) & (core == cc)))
            def _():
                z_copy(u, cc).start()
        return carry

    lax.fori_loop(0, LEAD, z_send, 0)
    xg[OWN, 4 * x + y, core] = disp[ep]

    l_trig.wait()
    l_q.wait()
    l_k.wait()
    l_v.wait()
    group = y // 2
    lane = lax.broadcasted_iota(jnp.int32, (WINDOW, 128), 1)
    first = lane < HD

    def rotate_block(n, carry):
        rows = pl.ds(pl.multiple_of(n * WINDOW, WINDOW), WINDOW)
        q = q_v[:, rows].astype(f32)
        k = k_v[rows, :].astype(f32)
        v = v_v[rows, :].astype(f32)
        k = jnp.where(group == 0, pltpu.roll(k, HD, 1), k)
        v = jnp.where(group == 0, pltpu.roll(v, HD, 1), v)
        both = jnp.where(first, jnp.concatenate([q, q], axis=0).T, k)
        block = ep * 4 + n
        cb = trig_v[2, pl.ds(block, 1), :]
        sb = trig_v[3, pl.ds(block, 1), :]
        cr = trig_v[0]
        sr = trig_v[1]
        cos = cb * cr - sb * sr
        sin = sb * cr + cb * sr
        swapped = jnp.where(lane % HD < HD // 2, pltpu.roll(both, 128 - HD // 2, 1), pltpu.roll(both, HD // 2, 1))
        turned = both * cos + swapped * sin
        qp[n] = jnp.where(first, turned, 0.0).astype(bf16)
        kv[n + 1] = jnp.where(first, pltpu.roll(turned, HD, 1), v).astype(bf16)
        return carry

    lax.fori_loop(0, 4, rotate_block, 0)
    rim = pltpu.make_async_remote_copy(
        src_ref=kv.at[4], dst_ref=kv.at[0], send_sem=rims.at[0], recv_sem=rimr.at[0],
        device_id=((ep + 1) % 32, y, x), device_id_type=MESH,
    )
    rim.start()

    l_ow.wait()

    def spread(h, carry):
        w = ow_v[pl.ds(pl.multiple_of(h * HD, HD), HD), :]
        zero = jnp.zeros((HD, 128), bf16)
        w01[pl.ds(pl.multiple_of(h * 128, 128), HD), :] = jnp.concatenate([w, zero], axis=1)
        w01[pl.ds(pl.multiple_of(h * 128 + HD, HD), HD), :] = jnp.concatenate([zero, w], axis=1)
        return carry

    lax.fori_loop(0, HEADS, spread, 0)

    sink = sink_ref[0]
    q_pos = lax.broadcasted_iota(jnp.int32, (WINDOW, 2 * WINDOW), 0) + WINDOW
    k_pos = lax.broadcasted_iota(jnp.int32, (WINDOW, 2 * WINDOW), 1)
    banded = (q_pos >= k_pos) & (q_pos - k_pos < WINDOW)

    def mix_of(n):
        keys = kv[pl.ds(n, 2)].reshape(2 * WINDOW, 128)
        scores = lax.dot_general(qp[n], keys, (((1,), (1,)), ((), ())), preferred_element_type=f32) * HD ** (-0.5)
        allowed = banded & ((ep * 4 + n) * WINDOW + k_pos >= WINDOW)
        scores = jnp.where(allowed, scores, mask_value)
        top = jnp.maximum(jnp.max(scores, axis=1, keepdims=True), sink)
        e = jnp.exp(scores - top)
        total = jnp.sum(e, axis=1, keepdims=True) + jnp.exp(sink - top)
        return dot((e / total).astype(bf16), keys)

    def attend(n):
        mixed = jnp.where(first, pltpu.roll(mix_of(n), HD, 1), mix_of(n + 2)).astype(bf16)
        xg[UNITS + 2 * n, 4 * y + x] = mixed[:ROWS].reshape(2, SLOTS, 128)
        xg[UNITS + 2 * n + 1, 4 * x + y] = mixed[ROWS:].reshape(2, SLOTS, 128)

    def ag1_copy(u, k):
        i, j = place(u)
        return pltpu.make_async_remote_copy(
            src_ref=xg.at[u, 4 * i + j], dst_ref=xg.at[u, 4 * i + j],
            send_sem=ags.at[u], recv_sem=a1r.at[u],
            device_id=along_j(u, k), device_id_type=MESH,
        )

    def ag3_copy(u, side):
        i, j = place(u)
        return pltpu.make_async_remote_copy(
            src_ref=xg.at[u, pl.ds(4 * i, 4)], dst_ref=xg.at[u, pl.ds(4 * i, 4)],
            send_sem=ags.at[u], recv_sem=(a4r if side else a3r).at[u],
            device_id=along_i(u, bw if side else fw), device_id_type=MESH,
        )

    def ag4_copy(u):
        i, j = place(u)
        row = (i + bw) % 4
        return pltpu.make_async_remote_copy(
            src_ref=xg.at[u, pl.ds(4 * row, 4)], dst_ref=xg.at[u, pl.ds(4 * row, 4)],
            send_sem=ags.at[u], recv_sem=a4r.at[u],
            device_id=along_i(u, fw), device_id_type=MESH,
        )

    def gathered(u):
        odd = u % 2
        tiles = []
        for yy in range(4):
            for xx in range(4):
                a = jnp.where(odd == 1, xx, yy)
                b = jnp.where(odd == 1, yy, xx)
                tiles.append(xg[u, 4 * a + b].reshape(ROWS, 128))
        return jnp.concatenate(tiles, axis=1)

    def rs1_copy(u, side):
        i, j = place(u)
        dest = (j + (bw if side else 2)) % 4
        return pltpu.make_async_remote_copy(
            src_ref=yb.at[u, dest], dst_ref=(rb if side else ra).at[u],
            send_sem=rss.at[u], recv_sem=(b2r if side else b1r).at[u],
            device_id=along_j(u, bw if side else fw), device_id_type=MESH,
        )

    def rs2_copy(u):
        return pltpu.make_async_remote_copy(
            src_ref=tb.at[u], dst_ref=rc.at[u], send_sem=rss.at[u], recv_sem=b2r.at[u],
            device_id=along_j(u, fw), device_id_type=MESH,
        )

    def rs3_copy(u, k):
        i, j = place(u)
        return pltpu.make_async_remote_copy(
            src_ref=qb.at[u, (i + k) % 4], dst_ref=rd.at[u, k - 1],
            send_sem=rss.at[u], recv_sem=b3r.at[u],
            device_id=along_i(u, k), device_id_type=MESH,
        )

    def home_copy(u, cc):
        dest = ((z + unit_dz(u) + NZ) % NZ) * 2 + cc
        return pltpu.make_async_remote_copy(
            src_ref=fb.at[u, cc], dst_ref=home.at[ep],
            send_sem=hs.at[0], recv_sem=hr.at[0],
            device_id=(dest, y, x), device_id_type=MESH,
        )

    def not_own(u, cc):
        return jnp.logical_not((u == OWN) & (core == cc))

    def tick(t, carry):
        u1 = t

        @pl.when(t == ATTEND[0])
        def _():
            rim.wait_recv()
            attend(0)

        @pl.when(t == ATTEND[1])
        def _():
            attend(1)

        @pl.when(t + LEAD < UNITS)
        def _():
            z_send(t + LEAD, 0)

        @pl.when(u1 < ALL_UNITS)
        def _():
            @pl.when(u1 < UNITS)
            def _():
                z_wait(u1)
            for k in (1, 2, 3):
                ag1_copy(u1, k).start()

        u2 = t - RS2

        @pl.when((u2 >= 0) & (u2 < UNITS))
        def _():
            i, j = place(u2)
            got(ra.at[u2], b1r.at[u2])
            tb[u2] = (ra[u2].astype(f32) + yb[u2, (j + fw) % 4].astype(f32)).astype(bf16)
            rs2_copy(u2).start()

        u3 = t - AG3

        @pl.when((u3 >= 0) & (u3 < ALL_UNITS))
        def _():
            got(xg.at[u3, pl.ds(0, 3)], a1r.at[u3])
            ag3_copy(u3, 0).start()
            ag3_copy(u3, 1).start()

        u4 = t - AG4

        @pl.when((u4 >= 0) & (u4 < ALL_UNITS))
        def _():
            got(xg.at[u4, pl.ds(0, 4)], a3r.at[u4])
            ag4_copy(u4).start()

        u5 = t - RS3

        @pl.when((u5 >= 0) & (u5 < UNITS))
        def _():
            i, j = place(u5)
            got(xg.at[u5, pl.ds(0, 8)], b2r.at[u5])
            qb[u5] = (yb[u5, j].astype(f32) + rc[u5].astype(f32) + rb[u5].astype(f32)).astype(bf16)
            for k in (1, 2, 3):
                rs3_copy(u5, k).start()

        u6 = t - FIN

        @pl.when((u6 >= 0) & (u6 < UNITS))
        def _():
            i, j = place(u6)
            got(rd.at[u6], b3r.at[u6])
            total = qb[u6, i].astype(f32) + rd[u6, 0].astype(f32) + rd[u6, 1].astype(f32) + rd[u6, 2].astype(f32)
            fb[u6] = total.astype(bf16).reshape(2, SLOTS, 128)
            for cc in (0, 1):
                @pl.when(not_own(u6, cc))
                def _():
                    home_copy(u6, cc).start()

                @pl.when(jnp.logical_not(not_own(u6, cc)))
                def _():
                    home[ep] = fb[u6, cc]

        um = t - MM

        @pl.when(um == 0)
        def _():
            l_wg.wait()
            l_wu.wait()
            l_wd.wait()

        @pl.when((um >= 0) & (um < ALL_UNITS))
        def _():
            got(xg.at[um, pl.ds(0, 8)], a4r.at[um])

        @pl.when((um >= 0) & (um < UNITS))
        def _():
            i, j = place(um)
            odd = um % 2
            rows_in = gathered(um)
            gate = dot(rows_in, wg_v[...])
            up = dot(rows_in, wu_v[...])
            hidden = (gate / (1.0 + jnp.exp(-gate)) * up).astype(bf16)
            for yy in range(4):
                part = dot(hidden, wd_v[:, yy * 512:(yy + 1) * 512]).astype(bf16)
                for xx in range(4):
                    a = jnp.where(odd == 1, yy, xx)
                    b = jnp.where(odd == 1, xx, yy)
                    yb[um, a, b] = part[:, xx * 128:(xx + 1) * 128]
            rs1_copy(um, 0).start()
            rs1_copy(um, 1).start()

        @pl.when((um >= UNITS) & (um < ALL_UNITS))
        def _():
            out = dot(gathered(um), w01[...]).astype(bf16)
            row = (um - UNITS) * ROWS
            attn_ref[pl.ds(pl.multiple_of(row, ROWS), ROWS), :] = out[:, :128]
            attn_ref[pl.ds(pl.multiple_of(row + 256, ROWS), ROWS), :] = out[:, 128:]

        @pl.when((u6 >= 0) & (u6 < ALL_UNITS))
        def _():
            left(xg.at[u6, pl.ds(0, 15)], ags.at[u6])

        @pl.when((u6 >= 0) & (u6 < UNITS))
        def _():
            left(xg.at[u6, pl.ds(0, 15)], rss.at[u6])

        return carry

    lax.fori_loop(0, ALL_UNITS + FIN, tick, 0)

    l_rw.wait()
    eye = t_col == t_row

    def as_column(row):
        return jnp.sum(jnp.where(eye, row, 0.0), axis=1, keepdims=True)

    weight0 = as_column(rw_v[0:1, :])
    weight1 = as_column(rw_v[1:2, :])
    slot0 = as_column(slot_row0)
    slot1 = as_column(slot_row1)
    slot_lane = lax.broadcasted_iota(jnp.int32, (TOK_E, EXPERTS * SLOTS), 1).astype(f32)
    pick0 = (slot_lane == slot0).astype(f32).astype(bf16)
    pick1 = (slot_lane == slot1).astype(f32).astype(bf16)

    got(home.at[pl.ds(0, EXPERTS - 1)], hr.at[0])
    left(home.at[pl.ds(0, EXPERTS - 1)], hs.at[0])
    left(disp.at[pl.ds(0, EXPERTS - 1)], zs.at[0])
    rim.wait_send()
    results = home[...].reshape(EXPERTS * SLOTS, 128)
    combined = dot(pick0, results) * weight0 + dot(pick1, results) * weight1
    eout_ref[...] = combined.astype(bf16)


def local(
    queries,
    keys,
    values,
    sink_logits,
    out_weight,
    expert_input,
    norm_gain,
    routes,
    route_weights,
    gate_weight,
    up_weight,
    down_weight,
):
    any_spec = pl.BlockSpec(memory_space=pl.ANY)
    vmem = pl.BlockSpec(memory_space=pltpu.VMEM)
    smem = pl.BlockSpec(memory_space=pltpu.SMEM)
    dma = pltpu.SemaphoreType.DMA
    trig = jnp.asarray(rope_tables())
    return pl.pallas_call(
        kernel,
        out_shape=(
            pltpu.VMEM((TOK_A, 128), bf16),
            pltpu.VMEM((TOK_E, 128), bf16),
        ),
        in_specs=[any_spec] * 3 + [smem] + [any_spec] * 9,
        out_specs=(vmem, vmem),
        scratch_shapes=[
            pltpu.VMEM((HD, TOK_A), bf16),
            pltpu.VMEM((TOK_A, 128), bf16),
            pltpu.VMEM((TOK_A, 128), bf16),
            pltpu.VMEM((HEADS * HD, 128), bf16),
            pltpu.VMEM((TOK_E, D), bf16),
            pltpu.VMEM((1, D), f32),
            pltpu.VMEM((2, TOK_E), jnp.int32),
            pltpu.VMEM((2, TOK_E), f32),
            pltpu.VMEM((D, FF_HERE), bf16),
            pltpu.VMEM((D, FF_HERE), bf16),
            pltpu.VMEM((FF_HERE, D), bf16),
            pltpu.VMEM((4, 128, 128), f32),
            pltpu.VMEM((EXPERTS, SLOTS, 128), bf16),
            pltpu.VMEM((D, 256), bf16),
            pltpu.VMEM((4, WINDOW, 128), bf16),
            pltpu.VMEM((5, WINDOW, 128), bf16),
            pltpu.VMEM((ALL_UNITS, 16, 2, SLOTS, 128), bf16),
            pltpu.VMEM((UNITS, 4, 4, ROWS, 128), bf16),
            pltpu.VMEM((UNITS, 4, ROWS, 128), bf16),
            pltpu.VMEM((UNITS, 4, ROWS, 128), bf16),
            pltpu.VMEM((UNITS, 4, ROWS, 128), bf16),
            pltpu.VMEM((UNITS, 4, ROWS, 128), bf16),
            pltpu.VMEM((UNITS, 4, ROWS, 128), bf16),
            pltpu.VMEM((UNITS, 3, ROWS, 128), bf16),
            pltpu.VMEM((UNITS, 2, SLOTS, 128), bf16),
            pltpu.VMEM((EXPERTS, SLOTS, 128), bf16),
            dma((12,)),
            dma((1,)),
            dma((UNITS,)),
            dma((1,)),
            dma((1,)),
            dma((ALL_UNITS,)),
            dma((ALL_UNITS,)),
            dma((ALL_UNITS,)),
            dma((ALL_UNITS,)),
            dma((UNITS,)),
            dma((UNITS,)),
            dma((UNITS,)),
            dma((UNITS,)),
            dma((1,)),
            dma((1,)),
        ],
        compiler_params=pltpu.CompilerParams(
            collective_id=0, has_side_effects=True, vmem_limit_bytes=63 * 1024 * 1024 + 512 * 1024
        ),
    )(
        queries.T, keys, values, sink_logits, out_weight, expert_input, norm_gain.reshape(1, D), routes.T, route_weights.T,
        gate_weight[0], up_weight[0], down_weight[0], trig,
    )


def solution(mesh):
    finer = Mesh(mesh.devices.reshape(mesh.shape["ep"], 4, 4), ("ep", "tp_0", "tp_1"))
    return jax.shard_map(
        local,
        mesh=finer,
        in_specs=(
            P("ep", TP),
            P("ep", None),
            P("ep", None),
            P(TP),
            P(None, TP),
            P("ep", None),
            P(),
            P("ep", None),
            P("ep", None),
            P("ep", None, TP),
            P("ep", None, TP),
            P("ep", TP, None),
        ),
        out_specs=(P("ep", TP), P("ep", TP)),
        check_vma=False,
    )
```

```python
import jax
import jax.numpy as jnp
import numpy as np
from jax import lax
from jax.experimental import pallas as pl
from jax.experimental.pallas import tpu as pltpu
from jax.sharding import Mesh
from jax.sharding import PartitionSpec as P

HEADS = 16
KV = 2
HD = 64
WINDOW = 128
TP = ("tp_0", "tp_1")
NZ = 16
UNITS = 16
ATT_UNITS = 4
ALL_UNITS = UNITS + ATT_UNITS
SLOTS = 32
EXPERTS = 32
ROWS = 64
D = 2048
FF_HERE = 256
TOK_E = 256
TOK_A = 512
MESH = pl.DeviceIdType.MESH
OWN = 15
LEAD = 5
ATTEND = (11, 13)

AG3, AG4, MM, RS2, RS3, FIN = 3, 6, 9, 12, 15, 18

rms_eps = 1e-06
mask_value = -1e30

f32 = jnp.float32
bf16 = jnp.bfloat16


def unit_dz(u):
    sign = 1 - 2 * (u % 2)
    out = jnp.where(u == 10, 8, (2 + u // 2) * sign)
    back = jnp.where(u == OWN, 0, jnp.where(u < 13, -7 * sign, -1 * sign))
    return jnp.where(u < 11, out, back)


def rope_tables():
    lane = np.arange(128) % 32
    freq = 10000.0 ** (-lane * (2.0 / HD))
    sign = np.where(np.arange(128) % 64 < 32, -1.0, 1.0)
    near = np.arange(WINDOW)[:, None] * freq[None, :]
    far = (np.arange(128) * WINDOW)[:, None] * freq[None, :]
    tables = np.stack([np.cos(near), np.sin(near) * sign, np.cos(far), np.sin(far) * sign])
    return tables.astype(np.float32)


def dot(a, b):
    return jnp.dot(a, b, preferred_element_type=f32)


def kernel(
    q_in, k_in, v_in, sink_ref, ow_in, x_in, gain_in, routes_in, rw_in, wg_in, wu_in, wd_in, trig_in,
    attn_ref, eout_ref,
    q_v, k_v, v_v, ow_v, x_v, gain_v, routes_v, rw_v, wg_v, wu_v, wd_v, trig_v,
    disp, w01, qp, kv, xg, yb, ra, rb, rc, tb, qb, rd, fb, home,
    in_sem, zs, zr, hs, hr, ags, a1r, a3r, a4r, rss, b1r, b2r, b3r, rims, rimr,
):
    ep = lax.axis_index("ep")
    y = lax.axis_index("tp_0")
    x = lax.axis_index("tp_1")
    z = ep // 2
    core = ep % 2
    tp = y * 4 + x
    sg = 1 - 2 * core

    barrier = pltpu.get_barrier_semaphore()

    for step in sorted(range(1, 32), key=lambda n: -min(n, 32 - n)):
        pl.semaphore_signal(barrier, inc=1, device_id=((ep + step) % 32, y, x), device_id_type=MESH)
    for k in (1, 2, 3):
        pl.semaphore_signal(barrier, inc=1, device_id=(ep, (y + k) % 4, x), device_id_type=MESH)
        pl.semaphore_signal(barrier, inc=1, device_id=(ep, y, (x + k) % 4), device_id_type=MESH)

    pairs = [
        (routes_in, routes_v), (x_in, x_v), (gain_in, gain_v), (rw_in, rw_v), (trig_in, trig_v), (q_in, q_v),
        (k_in, k_v), (v_in, v_v), (wg_in, wg_v), (wu_in, wu_v), (wd_in, wd_v), (ow_in, ow_v),
    ]
    loads = [pltpu.make_async_copy(a, b, in_sem.at[n]) for n, (a, b) in enumerate(pairs)]
    for load in loads:
        load.start()
    (l_routes, l_x, l_gain, l_rw, l_trig, l_q, l_k, l_v, l_wg, l_wu, l_wd, l_ow) = loads

    l_routes.wait()
    e_iota = lax.broadcasted_iota(jnp.int32, (EXPERTS, TOK_E), 0)
    one0 = (routes_v[0:1, :] == e_iota).astype(f32)
    one1 = (routes_v[1:2, :] == e_iota).astype(f32)
    t_row = lax.broadcasted_iota(jnp.int32, (TOK_E, TOK_E), 0)
    t_col = lax.broadcasted_iota(jnp.int32, (TOK_E, TOK_E), 1)
    before = (t_row < t_col).astype(f32).astype(bf16)
    place_of = dot((one0 + one1).astype(bf16), before) + (e_iota * SLOTS).astype(f32)
    slot_row0 = jnp.sum(one0 * place_of, axis=0, keepdims=True)
    slot_row1 = jnp.sum(one1 * place_of, axis=0, keepdims=True)

    l_x.wait()
    l_gain.wait()
    own_cols = pl.ds(pl.multiple_of(tp * 128, 128), 128)
    gain = gain_v[:, own_cols]

    squares = jnp.zeros((TOK_E, 128), f32)
    for n in range(D // 128):
        wide = x_v[:, n * 128:(n + 1) * 128].astype(f32)
        squares = squares + wide * wide
    inv = lax.rsqrt(jnp.sum(squares, axis=1, keepdims=True) * (1.0 / D) + rms_eps)
    normed = (x_v[:, own_cols].astype(f32) * inv * gain).astype(bf16)

    def fill_slots(n, carry):
        slot = (lax.broadcasted_iota(jnp.int32, (256, TOK_E), 0) + n * 256).astype(f32)
        pick = ((slot == slot_row0) | (slot == slot_row1)).astype(f32).astype(bf16)
        disp[pl.ds(n * 8, 8)] = dot(pick, normed).astype(bf16).reshape(8, SLOTS, 128)
        return carry

    lax.fori_loop(0, 4, fill_slots, 0)
    pl.semaphore_wait(barrier, 37)

    def place(u, of=core):
        odd = (u + of) % 2
        return jnp.where(odd == 1, x, y), jnp.where(odd == 1, y, x)

    def along_j(u, k):
        odd = (u + core) % 2
        return (ep, jnp.where(odd == 1, (y + k) % 4, y), jnp.where(odd == 1, x, (x + k) % 4))

    def along_i(u, k):
        odd = (u + core) % 2
        return (ep, jnp.where(odd == 1, y, (y + k) % 4), jnp.where(odd == 1, (x + k) % 4, x))

    fw = sg + 4
    bw = 4 - sg

    def got(like, sem):
        pltpu.make_async_remote_copy(
            src_ref=like, dst_ref=like, send_sem=rims.at[0], recv_sem=sem,
            device_id=(ep ^ 1, y, x), device_id_type=MESH,
        ).wait_recv()

    def left(like, sem):
        pltpu.make_async_remote_copy(
            src_ref=like, dst_ref=like, send_sem=sem, recv_sem=rimr.at[0],
            device_id=(ep ^ 1, y, x), device_id_type=MESH,
        ).wait_send()

    def z_copy(u, cc):
        dest = ((z - unit_dz(u) + NZ) % NZ) * 2 + cc
        i, j = place(u, cc)
        return pltpu.make_async_remote_copy(
            src_ref=disp.at[dest], dst_ref=xg.at[u, 4 * i + j, core],
            send_sem=zs.at[0], recv_sem=zr.at[u],
            device_id=(dest, y, x), device_id_type=MESH,
        )

    def z_wait(u):
        i, j = place(u)

        @pl.when(u != OWN)
        def _():
            got(xg.at[u, 4 * i + j], zr.at[u])

        @pl.when(u == OWN)
        def _():
            got(xg.at[u, 4 * i + j, 1 - core], zr.at[u])

    def z_send(u, carry):
        for cc in (0, 1):
            @pl.when(jnp.logical_not((u == OWN) & (core == cc)))
            def _():
                z_copy(u, cc).start()
        return carry

    lax.fori_loop(0, LEAD, z_send, 0)
    own_i, own_j = place(OWN)
    xg[OWN, 4 * own_i + own_j, core] = disp[ep]

    l_trig.wait()
    l_q.wait()
    l_k.wait()
    l_v.wait()
    group = y // 2
    lane = lax.broadcasted_iota(jnp.int32, (WINDOW, 128), 1)
    first = lane < HD

    def rotate_block(n, carry):
        rows = pl.ds(pl.multiple_of(n * WINDOW, WINDOW), WINDOW)
        q = q_v[:, rows].astype(f32)
        k = k_v[rows, :].astype(f32)
        v = v_v[rows, :].astype(f32)
        k = jnp.where(group == 0, pltpu.roll(k, HD, 1), k)
        v = jnp.where(group == 0, pltpu.roll(v, HD, 1), v)
        both = jnp.where(first, jnp.concatenate([q, q], axis=0).T, k)
        block = ep * 4 + n
        cb = trig_v[2, pl.ds(block, 1), :]
        sb = trig_v[3, pl.ds(block, 1), :]
        cr = trig_v[0]
        sr = trig_v[1]
        cos = cb * cr - sb * sr
        sin = sb * cr + cb * sr
        swapped = jnp.where(lane % HD < HD // 2, pltpu.roll(both, 128 - HD // 2, 1), pltpu.roll(both, HD // 2, 1))
        turned = both * cos + swapped * sin
        qp[n] = jnp.where(first, turned, 0.0).astype(bf16)
        kv[n + 1] = jnp.where(first, pltpu.roll(turned, HD, 1), v).astype(bf16)
        return carry

    lax.fori_loop(0, 4, rotate_block, 0)
    rim = pltpu.make_async_remote_copy(
        src_ref=kv.at[4], dst_ref=kv.at[0], send_sem=rims.at[0], recv_sem=rimr.at[0],
        device_id=((ep + 1) % 32, y, x), device_id_type=MESH,
    )
    rim.start()

    l_ow.wait()

    def spread(h, carry):
        w = ow_v[pl.ds(pl.multiple_of(h * HD, HD), HD), :]
        zero = jnp.zeros((HD, 128), bf16)
        w01[pl.ds(pl.multiple_of(h * 128, 128), HD), :] = jnp.concatenate([w, zero], axis=1)
        w01[pl.ds(pl.multiple_of(h * 128 + HD, HD), HD), :] = jnp.concatenate([zero, w], axis=1)
        return carry

    lax.fori_loop(0, HEADS, spread, 0)

    sink = sink_ref[0]
    q_pos = lax.broadcasted_iota(jnp.int32, (WINDOW, 2 * WINDOW), 0) + WINDOW
    k_pos = lax.broadcasted_iota(jnp.int32, (WINDOW, 2 * WINDOW), 1)
    banded = (q_pos >= k_pos) & (q_pos - k_pos < WINDOW)

    def mix_of(n):
        keys = kv[pl.ds(n, 2)].reshape(2 * WINDOW, 128)
        scores = lax.dot_general(qp[n], keys, (((1,), (1,)), ((), ())), preferred_element_type=f32) * HD ** (-0.5)
        allowed = banded & ((ep * 4 + n) * WINDOW + k_pos >= WINDOW)
        scores = jnp.where(allowed, scores, mask_value)
        top = jnp.maximum(jnp.max(scores, axis=1, keepdims=True), sink)
        e = jnp.exp(scores - top)
        total = jnp.sum(e, axis=1, keepdims=True) + jnp.exp(sink - top)
        return dot((e / total).astype(bf16), keys)

    def attend(n):
        mixed = jnp.where(first, pltpu.roll(mix_of(n), HD, 1), mix_of(n + 2)).astype(bf16)
        i, j = place(0)
        xg[UNITS + 2 * n, 4 * i + j] = mixed[:ROWS].reshape(2, SLOTS, 128)
        xg[UNITS + 2 * n + 1, 4 * j + i] = mixed[ROWS:].reshape(2, SLOTS, 128)

    def ag1_copy(u, k):
        i, j = place(u)
        return pltpu.make_async_remote_copy(
            src_ref=xg.at[u, 4 * i + j], dst_ref=xg.at[u, 4 * i + j],
            send_sem=ags.at[u], recv_sem=a1r.at[u],
            device_id=along_j(u, k), device_id_type=MESH,
        )

    def ag3_copy(u, side):
        i, j = place(u)
        return pltpu.make_async_remote_copy(
            src_ref=xg.at[u, pl.ds(4 * i, 4)], dst_ref=xg.at[u, pl.ds(4 * i, 4)],
            send_sem=ags.at[u], recv_sem=(a4r if side else a3r).at[u],
            device_id=along_i(u, bw if side else fw), device_id_type=MESH,
        )

    def ag4_copy(u):
        i, j = place(u)
        row = (i + bw) % 4
        return pltpu.make_async_remote_copy(
            src_ref=xg.at[u, pl.ds(4 * row, 4)], dst_ref=xg.at[u, pl.ds(4 * row, 4)],
            send_sem=ags.at[u], recv_sem=a4r.at[u],
            device_id=along_i(u, fw), device_id_type=MESH,
        )

    def gathered(u):
        odd = (u + core) % 2
        tiles = []
        for yy in range(4):
            for xx in range(4):
                a = jnp.where(odd == 1, xx, yy)
                b = jnp.where(odd == 1, yy, xx)
                tiles.append(xg[u, 4 * a + b].reshape(ROWS, 128))
        return jnp.concatenate(tiles, axis=1)

    def rs1_copy(u, side):
        i, j = place(u)
        dest = (j + (bw if side else 2)) % 4
        return pltpu.make_async_remote_copy(
            src_ref=yb.at[u, dest], dst_ref=(rb if side else ra).at[u],
            send_sem=rss.at[u], recv_sem=(b2r if side else b1r).at[u],
            device_id=along_j(u, bw if side else fw), device_id_type=MESH,
        )

    def rs2_copy(u):
        return pltpu.make_async_remote_copy(
            src_ref=tb.at[u], dst_ref=rc.at[u], send_sem=rss.at[u], recv_sem=b2r.at[u],
            device_id=along_j(u, fw), device_id_type=MESH,
        )

    def rs3_copy(u, k):
        i, j = place(u)
        return pltpu.make_async_remote_copy(
            src_ref=qb.at[u, (i + k) % 4], dst_ref=rd.at[u, k - 1],
            send_sem=rss.at[u], recv_sem=b3r.at[u],
            device_id=along_i(u, k), device_id_type=MESH,
        )

    def home_copy(u, cc):
        dest = ((z + unit_dz(u) + NZ) % NZ) * 2 + cc
        return pltpu.make_async_remote_copy(
            src_ref=fb.at[u, cc], dst_ref=home.at[ep],
            send_sem=hs.at[0], recv_sem=hr.at[0],
            device_id=(dest, y, x), device_id_type=MESH,
        )

    def not_own(u, cc):
        return jnp.logical_not((u == OWN) & (core == cc))

    def tick(t, carry):
        u1 = t

        @pl.when(t == ATTEND[0])
        def _():
            rim.wait_recv()
            attend(0)

        @pl.when(t == ATTEND[1])
        def _():
            attend(1)

        @pl.when(t + LEAD < UNITS)
        def _():
            z_send(t + LEAD, 0)

        @pl.when(u1 < ALL_UNITS)
        def _():
            @pl.when(u1 < UNITS)
            def _():
                z_wait(u1)
            for k in (1, 2, 3):
                ag1_copy(u1, k).start()

        u2 = t - RS2

        @pl.when((u2 >= 0) & (u2 < UNITS))
        def _():
            i, j = place(u2)
            got(ra.at[u2], b1r.at[u2])
            tb[u2] = (ra[u2].astype(f32) + yb[u2, (j + fw) % 4].astype(f32)).astype(bf16)
            rs2_copy(u2).start()

        u3 = t - AG3

        @pl.when((u3 >= 0) & (u3 < ALL_UNITS))
        def _():
            got(xg.at[u3, pl.ds(0, 3)], a1r.at[u3])
            ag3_copy(u3, 0).start()
            ag3_copy(u3, 1).start()

        u4 = t - AG4

        @pl.when((u4 >= 0) & (u4 < ALL_UNITS))
        def _():
            got(xg.at[u4, pl.ds(0, 4)], a3r.at[u4])
            ag4_copy(u4).start()

        u5 = t - RS3

        @pl.when((u5 >= 0) & (u5 < UNITS))
        def _():
            i, j = place(u5)
            got(xg.at[u5, pl.ds(0, 8)], b2r.at[u5])
            qb[u5] = (yb[u5, j].astype(f32) + rc[u5].astype(f32) + rb[u5].astype(f32)).astype(bf16)
            for k in (1, 2, 3):
                rs3_copy(u5, k).start()

        u6 = t - FIN

        @pl.when((u6 >= 0) & (u6 < UNITS))
        def _():
            i, j = place(u6)
            got(rd.at[u6], b3r.at[u6])
            total = qb[u6, i].astype(f32) + rd[u6, 0].astype(f32) + rd[u6, 1].astype(f32) + rd[u6, 2].astype(f32)
            fb[u6] = total.astype(bf16).reshape(2, SLOTS, 128)
            for cc in (0, 1):
                @pl.when(not_own(u6, cc))
                def _():
                    home_copy(u6, cc).start()

                @pl.when(jnp.logical_not(not_own(u6, cc)))
                def _():
                    home[ep] = fb[u6, cc]

        um = t - MM

        @pl.when(um == 0)
        def _():
            l_wg.wait()
            l_wu.wait()
            l_wd.wait()

        @pl.when((um >= 0) & (um < ALL_UNITS))
        def _():
            got(xg.at[um, pl.ds(0, 8)], a4r.at[um])

        @pl.when((um >= 0) & (um < UNITS))
        def _():
            i, j = place(um)
            odd = (um + core) % 2
            rows_in = gathered(um)
            gate = dot(rows_in, wg_v[...])
            up = dot(rows_in, wu_v[...])
            hidden = (gate / (1.0 + jnp.exp(-gate)) * up).astype(bf16)
            for yy in range(4):
                part = dot(hidden, wd_v[:, yy * 512:(yy + 1) * 512]).astype(bf16)
                for xx in range(4):
                    a = jnp.where(odd == 1, yy, xx)
                    b = jnp.where(odd == 1, xx, yy)
                    yb[um, a, b] = part[:, xx * 128:(xx + 1) * 128]
            rs1_copy(um, 0).start()
            rs1_copy(um, 1).start()

        @pl.when((um >= UNITS) & (um < ALL_UNITS))
        def _():
            out = dot(gathered(um), w01[...]).astype(bf16)
            row = (um - UNITS) * ROWS
            attn_ref[pl.ds(pl.multiple_of(row, ROWS), ROWS), :] = out[:, :128]
            attn_ref[pl.ds(pl.multiple_of(row + 256, ROWS), ROWS), :] = out[:, 128:]

        @pl.when((u6 >= 0) & (u6 < ALL_UNITS))
        def _():
            left(xg.at[u6, pl.ds(0, 15)], ags.at[u6])

        @pl.when((u6 >= 0) & (u6 < UNITS))
        def _():
            left(xg.at[u6, pl.ds(0, 15)], rss.at[u6])

        return carry

    lax.fori_loop(0, ALL_UNITS + FIN, tick, 0)

    l_rw.wait()
    eye = t_col == t_row

    def as_column(row):
        return jnp.sum(jnp.where(eye, row, 0.0), axis=1, keepdims=True)

    weight0 = as_column(rw_v[0:1, :])
    weight1 = as_column(rw_v[1:2, :])
    slot0 = as_column(slot_row0)
    slot1 = as_column(slot_row1)
    slot_lane = lax.broadcasted_iota(jnp.int32, (TOK_E, EXPERTS * SLOTS), 1).astype(f32)
    pick0 = (slot_lane == slot0).astype(f32).astype(bf16)
    pick1 = (slot_lane == slot1).astype(f32).astype(bf16)

    got(home.at[pl.ds(0, EXPERTS - 1)], hr.at[0])
    left(home.at[pl.ds(0, EXPERTS - 1)], hs.at[0])
    left(disp.at[pl.ds(0, EXPERTS - 1)], zs.at[0])
    rim.wait_send()
    results = home[...].reshape(EXPERTS * SLOTS, 128)
    combined = dot(pick0, results) * weight0 + dot(pick1, results) * weight1
    eout_ref[...] = combined.astype(bf16)


def local(
    queries,
    keys,
    values,
    sink_logits,
    out_weight,
    expert_input,
    norm_gain,
    routes,
    route_weights,
    gate_weight,
    up_weight,
    down_weight,
):
    any_spec = pl.BlockSpec(memory_space=pl.ANY)
    vmem = pl.BlockSpec(memory_space=pltpu.VMEM)
    smem = pl.BlockSpec(memory_space=pltpu.SMEM)
    dma = pltpu.SemaphoreType.DMA
    trig = jnp.asarray(rope_tables())
    return pl.pallas_call(
        kernel,
        out_shape=(
            pltpu.VMEM((TOK_A, 128), bf16),
            pltpu.VMEM((TOK_E, 128), bf16),
        ),
        in_specs=[any_spec] * 3 + [smem] + [any_spec] * 9,
        out_specs=(vmem, vmem),
        scratch_shapes=[
            pltpu.VMEM((HD, TOK_A), bf16),
            pltpu.VMEM((TOK_A, 128), bf16),
            pltpu.VMEM((TOK_A, 128), bf16),
            pltpu.VMEM((HEADS * HD, 128), bf16),
            pltpu.VMEM((TOK_E, D), bf16),
            pltpu.VMEM((1, D), f32),
            pltpu.VMEM((2, TOK_E), jnp.int32),
            pltpu.VMEM((2, TOK_E), f32),
            pltpu.VMEM((D, FF_HERE), bf16),
            pltpu.VMEM((D, FF_HERE), bf16),
            pltpu.VMEM((FF_HERE, D), bf16),
            pltpu.VMEM((4, 128, 128), f32),
            pltpu.VMEM((EXPERTS, SLOTS, 128), bf16),
            pltpu.VMEM((D, 256), bf16),
            pltpu.VMEM((4, WINDOW, 128), bf16),
            pltpu.VMEM((5, WINDOW, 128), bf16),
            pltpu.VMEM((ALL_UNITS, 16, 2, SLOTS, 128), bf16),
            pltpu.VMEM((UNITS, 4, 4, ROWS, 128), bf16),
            pltpu.VMEM((UNITS, 4, ROWS, 128), bf16),
            pltpu.VMEM((UNITS, 4, ROWS, 128), bf16),
            pltpu.VMEM((UNITS, 4, ROWS, 128), bf16),
            pltpu.VMEM((UNITS, 4, ROWS, 128), bf16),
            pltpu.VMEM((UNITS, 4, ROWS, 128), bf16),
            pltpu.VMEM((UNITS, 3, ROWS, 128), bf16),
            pltpu.VMEM((UNITS, 2, SLOTS, 128), bf16),
            pltpu.VMEM((EXPERTS, SLOTS, 128), bf16),
            dma((12,)),
            dma((1,)),
            dma((UNITS,)),
            dma((1,)),
            dma((1,)),
            dma((ALL_UNITS,)),
            dma((ALL_UNITS,)),
            dma((ALL_UNITS,)),
            dma((ALL_UNITS,)),
            dma((UNITS,)),
            dma((UNITS,)),
            dma((UNITS,)),
            dma((UNITS,)),
            dma((1,)),
            dma((1,)),
        ],
        compiler_params=pltpu.CompilerParams(
            collective_id=0, has_side_effects=True, vmem_limit_bytes=63 * 1024 * 1024 + 512 * 1024
        ),
    )(
        queries.T, keys, values, sink_logits, out_weight, expert_input, norm_gain.reshape(1, D), routes.T, route_weights.T,
        gate_weight[0], up_weight[0], down_weight[0], trig,
    )


def solution(mesh):
    finer = Mesh(mesh.devices.reshape(mesh.shape["ep"], 4, 4), ("ep", "tp_0", "tp_1"))
    return jax.shard_map(
        local,
        mesh=finer,
        in_specs=(
            P("ep", TP),
            P("ep", None),
            P("ep", None),
            P(TP),
            P(None, TP),
            P("ep", None),
            P(),
            P("ep", None),
            P("ep", None),
            P("ep", None, TP),
            P("ep", None, TP),
            P("ep", TP, None),
        ),
        out_specs=(P("ep", TP), P("ep", TP)),
        check_vma=False,
    )
```
